32 devices in a mesh: kv: 8 (over z, x), tp: 4 (over y, core).
Axes of the slice: x: 2, y: 2, z: 4, core: 2. Of those that a mesh axis runs over, the one named last changes fastest.
Arguments:
- inputs: bfloat16 [4, 2048, 2048], P(None, 'kv'), may hold values from -40 to 40
- query_weight: bfloat16 [2048, 2048], P(None, 'tp'), may hold values from -0.125 to 0.125
- key_weight: bfloat16 [2048, 1024], P(None, 'tp'), may hold values from -0.125 to 0.125
- value_weight: bfloat16 [2048, 1024], P(None, 'tp'), may hold values from -0.125 to 0.125
- out_weight: bfloat16 [2048, 2048], P('tp'), may hold values from -1 to 1
- chosen: int32 [4, 32, 32], P(None, 'kv'), may hold values from 0 to 31, as said below
- lengths: int32 [4], replicated, may hold values from 1 to 2048, 3072 in all
Outputs:
- mixed: bfloat16 [4, 2048, 2048], P(None, 'kv', 'tp')
The draws below stay inside these ranges and needn't reach their ends.
Inputs may be any that keep to these rules, and one draw needn't show every extreme that they name: chosen[b, q, 0] = q; every entry names a block of the same sequence at or before q; entries may repeat. Over the query blocks of positions k * 256 to (k+1) * 256 - 1 of all sequences, the named blocks that lie in another span of 256 positions number at most 3 distinct blocks for each other span, and 3 is reached.
All inputs are finite; a program needn't handle non-finite values.
Results may differ from the reference program's by a relative error of at most 0.014.
The reference program's roundings to bfloat16 on the way count: a program that leaves them out, or rounds other values in their place, can miss the bound.
Values may be sent and summed in bfloat16 or wider, within the bound.
No kernel may reach another device: no remote copies, remote signals or barrier semaphores. Data moves between devices by JAX's collectives and lax.ppermute only.
A program may use at most 128 MiB of HBM per device.

```python
import math
import jax
import jax.numpy as jnp
import numpy as np
from jax import lax

D = 2048
HEADS = 16
KV_HEADS = 8
HD = 128
KB = 64
TOPK = 32
CAP = 3
BATCH = 4
SEQ_DEV = 256
SEQ = 2048
NB = 32
N_TP = 4


def draw_inputs(key, part):
    key_base = jax.random.fold_in(jax.random.fold_in(key, 3), 0)
    entries = jax.random.normal(key_base, (BATCH, SEQ, D), jnp.float32)
    return jnp.clip(entries, -40.0, 40.0).astype(jnp.bfloat16)


def draw_chosen(key, part):
    per_dev = SEQ_DEV // KB
    ndevices = NB // per_dev
    owned = BATCH * per_dev
    key_count, key_rank, key_order = jax.random.split(jax.random.fold_in(key, 7), 3)
    receiver = jnp.arange(ndevices, dtype=jnp.int32)[:, None]
    sender = jnp.arange(ndevices, dtype=jnp.int32)[None, :]
    counts = jax.random.randint(key_count, (ndevices, ndevices), 1, CAP + 1)
    counts = jnp.where(sender == receiver - 1, CAP, counts)
    counts = jnp.where(sender < receiver, counts, 0)
    local_ids = jnp.arange(owned, dtype=jnp.int32)
    noise = jax.random.randint(key_rank, (ndevices, ndevices, owned), 0, 1 << 20) * owned + local_ids
    ranks = jnp.argsort(jnp.argsort(noise, axis=-1), axis=-1)
    picked = ranks < counts[:, :, None]
    order_noise = jax.random.randint(key_order, (ndevices, ndevices), 0, 1 << 20) * ndevices + sender
    priority = jnp.argsort(jnp.argsort(order_noise, axis=-1), axis=-1) + 2
    priority = jnp.where(sender == receiver - ndevices // 2, 1, priority)
    priority = jnp.where(sender == receiver - 1, 0, priority)
    seq_of = local_ids // per_dev
    global_block = sender[:, :, None] * per_dev + (local_ids % per_dev)[None, None, :]
    big_score = (ndevices + 4) * owned
    seq_range = jnp.arange(BATCH, dtype=jnp.int32)
    in_seq = picked[:, None, :, :] & (seq_of[None, None, None, :] == seq_range[None, :, None, None])
    scored = jnp.where(in_seq, priority[:, None, :, None] * owned + local_ids[None, None, None, :], big_score)
    scored = scored.reshape(ndevices, BATCH, ndevices * owned)
    sorted_idx = jnp.argsort(scored, axis=-1)
    pool_size = jnp.sum(in_seq.reshape(ndevices, BATCH, ndevices * owned).astype(jnp.int32), axis=-1)
    pool_blocks = jnp.take_along_axis(jnp.broadcast_to(global_block.reshape(1, 1, ndevices * owned), (ndevices, BATCH, ndevices * owned)), sorted_idx, axis=-1)
    local_row = jnp.arange(per_dev, dtype=jnp.int32)[:, None]
    slot_col = jnp.arange(TOPK, dtype=jnp.int32)[None, :]
    base_count = local_row * (TOPK - 1) - local_row * (local_row - 1) // 2
    counter = base_count + slot_col - 1 - local_row
    safe_size = jnp.maximum(pool_size, 1)
    pool_pick = jnp.take_along_axis(pool_blocks, counter.reshape(1, 1, -1) % safe_size[:, :, None], axis=-1)
    pool_pick = pool_pick.reshape(ndevices, BATCH, per_dev, TOPK)
    own_block = jnp.arange(ndevices, dtype=jnp.int32)[:, None, None, None] * per_dev + local_row[None, None, :, :] + 0 * slot_col[None, None, :, :]
    earlier = own_block - local_row[None, None, :, :] + slot_col[None, None, :, :] - 1
    result = jnp.where(pool_size[:, :, None, None] > 0, pool_pick, own_block)
    result = jnp.where((slot_col >= 1) & (slot_col <= local_row), earlier, result)
    result = jnp.where(slot_col == 0, own_block, result)
    return jnp.transpose(result, (1, 0, 2, 3)).reshape(BATCH, NB, TOPK).astype(jnp.int32)


def level_of(stream_key, dims, cuts, smallest, largest):
    level = 1.0
    for dim, parts in cuts:
        steps = jax.random.uniform(jax.random.fold_in(jax.random.fold_in(stream_key, 6), dim), (parts,), jnp.float32, smallest / len(cuts), largest / len(cuts))
        level = level * jnp.repeat(jnp.exp(steps), dims[dim] // parts).reshape((-1,) + (1,) * (len(dims) - 1 - dim))
    return level


def profile(count, total, reach, lean):
    portions = [(1 << 20) // math.isqrt(grade ** lean) + 1 for grade in range(2, count + 1)]
    surplus, given = total - reach - (count - 1), [1] * (count - 1)
    while surplus > 0:
        candidates = [i for i in range(count - 1) if given[i] < reach]
        mass, budget = sum([portions[i] for i in candidates]), surplus
        for i in candidates:
            addition = min(reach - given[i], max(1, budget * portions[i] // mass), surplus)
            given[i] = given[i] + addition
            surplus = surplus - addition
    return np.array([reach] + given)


def uneven(key, amount, total, bound, slope):
    if amount == 2:
        one = jax.random.randint(key, (), max(1, total - bound), min(bound, total - 1) + 1)
        return jnp.stack([one, total - one])
    tallies = jnp.asarray(profile(amount, total, bound, slope), jnp.int32)
    pairs = (amount - 1) // 2
    source_of, taker = tallies[1:1 + 2 * pairs:2], tallies[2:2 + 2 * pairs:2]
    margin = jnp.minimum(source_of - 1, bound - taker)
    moved = jax.random.randint(jax.random.fold_in(key, 1), (pairs,), 0, 1 << 20) % (margin + 1)
    tallies = tallies.at[1:1 + 2 * pairs:2].set(source_of - moved).at[2:2 + 2 * pairs:2].set(taker + moved)
    return tallies[jax.random.permutation(jax.random.fold_in(key, 2), amount)]


def gaussian(stream_key, extent, spread, bound, pieces=(), kind=jnp.bfloat16):
    array = jax.random.normal(stream_key, extent, jnp.float32) * spread
    if len(pieces) > 0:
        array = level_of(stream_key, extent, pieces, -0.22, 0.18) * array
    return jnp.clip(array, min=-bound, max=bound).astype(kind)


def setup_inputs(seed: int = 0) -> dict:
    seeds = jax.random.split(jax.random.key(seed), 8)
    return {
        "inputs": draw_inputs(jax.random.fold_in(seeds[7], 71), 0),
        "query_weight": gaussian(seeds[1], (D, HEADS * HD), D ** -0.5, 0.125, ((1, 4),)),
        "key_weight": gaussian(seeds[2], (D, KV_HEADS * HD), D ** -0.5, 0.125, ((1, 4),)),
        "value_weight": gaussian(seeds[3], (D, KV_HEADS * HD), D ** -0.5, 0.125, ((1, 4),)),
        "out_weight": gaussian(seeds[4], (HEADS * HD, D), (HEADS * HD // 64) ** -0.5, 1.0, ((0, 4),)),
        "chosen": draw_chosen(jax.random.fold_in(seeds[7], 71), 0),
        "lengths": uneven(seeds[6], BATCH, SEQ + SEQ // 2, SEQ, 2).astype(jnp.int32),
    }


def unique_slots(chosen_rows):
    order = jnp.arange(TOPK, dtype=jnp.int32)
    repeated = jnp.any((chosen_rows[..., :, None] == chosen_rows[..., None, :]) & (order[:, None] > order[None, :]), axis=-1)
    return jnp.repeat(jnp.logical_not(repeated), KB, axis=-1)


def attend(queries, key_sets, value_sets, key_pos, unique_key, query_pos, live_length):
    scores = jnp.einsum("nqkgd,npkd->nkgqp", queries.astype(jnp.float32), key_sets.astype(jnp.float32)) * (HD ** -0.5)
    allowed = (key_pos[:, None, :] <= query_pos[:, :, None]) & (key_pos[:, None, :] < live_length) & unique_key[:, None, :]
    allowed = allowed | (key_pos[:, None, :] == query_pos[:, :, None])
    scores = jnp.where(allowed[:, None, None], scores, -jnp.inf)
    highest = jnp.max(scores, axis=-1, keepdims=True)
    raised = jnp.exp(scores - highest)
    weights = (raised / jnp.sum(raised, axis=-1, keepdims=True)).astype(jnp.bfloat16)
    combined = jnp.einsum("nkgqp,npkd->nqkgd", weights.astype(jnp.float32), value_sets.astype(jnp.float32))
    living = (query_pos < live_length)[:, :, None, None, None]
    return jnp.where(living, combined, 0.0).astype(jnp.bfloat16)


def reference(inputs, query_weight, key_weight, value_weight, out_weight, chosen, lengths):
    per_group = HEADS // KV_HEADS
    flat_rows = inputs.reshape(BATCH * SEQ, D)
    queries = jnp.dot(flat_rows, query_weight, preferred_element_type=jnp.float32).astype(jnp.bfloat16)
    queries = queries.reshape(BATCH, NB, KB, KV_HEADS, per_group, HD)
    key_rows = jnp.dot(flat_rows, key_weight, preferred_element_type=jnp.float32).astype(jnp.bfloat16)
    key_rows = key_rows.reshape(BATCH, NB, KB, KV_HEADS, HD)
    value_rows = jnp.dot(flat_rows, value_weight, preferred_element_type=jnp.float32).astype(jnp.bfloat16)
    value_rows = value_rows.reshape(BATCH, NB, KB, KV_HEADS, HD)
    offsets = jnp.arange(KB, dtype=jnp.int32)

    def one_block(block_pair):
        seq_index, block_id = block_pair
        names = chosen[seq_index, block_id]
        key_sets = key_rows[seq_index][names].reshape(1, TOPK * KB, KV_HEADS, HD)
        value_sets = value_rows[seq_index][names].reshape(1, TOPK * KB, KV_HEADS, HD)
        key_pos = (names[:, None] * KB + offsets[None, :]).reshape(1, TOPK * KB)
        query_pos = (block_id * KB + offsets)[None, :]
        unique_key = unique_slots(names)[None, :]
        result = attend(queries[seq_index, block_id][None], key_sets, value_sets, key_pos, unique_key, query_pos, lengths[seq_index])
        return result[0]

    seq_ids = jnp.repeat(jnp.arange(BATCH, dtype=jnp.int32), NB)
    block_ids = jnp.tile(jnp.arange(NB, dtype=jnp.int32), BATCH)
    attended = lax.map(one_block, (seq_ids, block_ids)).reshape(BATCH * SEQ, HEADS * HD)
    group_width = HEADS * HD // N_TP
    summed = jnp.zeros((BATCH * SEQ, D), jnp.float32)
    for group_id in range(N_TP):
        partial_value = jnp.dot(attended[:, group_id * group_width:(group_id + 1) * group_width],
                          out_weight[group_id * group_width:(group_id + 1) * group_width],
                          preferred_element_type=jnp.float32).astype(jnp.bfloat16)
        summed = summed + lax.optimization_barrier(partial_value).astype(jnp.float32)
    return summed.astype(jnp.bfloat16).reshape(BATCH, SEQ, D)
```

```python
import functools
import math

import jax
import jax.numpy as jnp
from jax import lax
from jax.experimental import pallas as pl
from jax.experimental.pallas import tpu as pltpu
from jax.sharding import PartitionSpec as P

HD = 128
KB = 64
CORES = 2
LOG2E = math.log2(math.e)


def smem():
    return pl.BlockSpec(memory_space=pltpu.SMEM)


def first_kv(order, rows, wk, wv):
    _, span, width = rows.shape
    kv_width = wk.shape[1]
    tiles = 4
    depth = width // tiles

    def body(order_ref, x_ref, k_ref, v_ref, out_ref, acc):
        step = pl.program_id(0)

        @pl.when(step == 0)
        def _():
            acc[...] = jnp.zeros_like(acc)

        x = x_ref[0]
        acc[:, :kv_width] += jnp.dot(x, k_ref[...], preferred_element_type=jnp.float32)
        acc[:, kv_width:] += jnp.dot(x, v_ref[...], preferred_element_type=jnp.float32)

        @pl.when(step == tiles - 1)
        def _():
            out_ref[...] = acc[...].astype(out_ref.dtype)

    return pl.pallas_call(
        body,
        grid_spec=pltpu.PrefetchScalarGridSpec(
            num_scalar_prefetch=1,
            grid=(tiles,),
            in_specs=[
                pl.BlockSpec((1, span, depth), lambda s, order: (order[0], 0, s)),
                pl.BlockSpec((depth, kv_width), lambda s, order: (s, 0)),
                pl.BlockSpec((depth, kv_width), lambda s, order: (s, 0)),
            ],
            out_specs=pl.BlockSpec((span, 2 * kv_width), lambda s, order: (0, 0)),
            scratch_shapes=[pltpu.VMEM((span, 2 * kv_width), jnp.float32)],
        ),
        out_shape=jax.ShapeDtypeStruct((span, 2 * kv_width), jnp.bfloat16),
        cost_estimate=pl.CostEstimate(
            flops=4 * span * width * kv_width * 2, bytes_accessed=3 << 20, transcendentals=0
        ),
        name="first_kv",
    )(order, rows, wk, wv)


def other_qkv(order, live, rows, wq, wk, wv):
    batch, span, width = rows.shape
    kv_width = wk.shape[1]
    q_width = wq.shape[1]

    def body(order_ref, live_ref, x_ref, q_ref, k_ref, v_ref, q_out, kv_out):
        tier = pl.program_id(0)

        @pl.when(tier < live_ref[0])
        def _():
            x = x_ref[0]
            q_out[0] = jnp.dot(x, q_ref[...], preferred_element_type=jnp.float32).astype(
                q_out.dtype
            )

            @pl.when(tier > 0)
            def _():
                kv_out[0, :, :kv_width] = jnp.dot(
                    x, k_ref[...], preferred_element_type=jnp.float32
                ).astype(kv_out.dtype)
                kv_out[0, :, kv_width:] = jnp.dot(
                    x, v_ref[...], preferred_element_type=jnp.float32
                ).astype(kv_out.dtype)

    def row_index(tier, order, live):
        return (order[jnp.minimum(tier, jnp.maximum(live[0] - 1, 0))], 0, 0)

    whole = lambda tier, order, live: (0, 0)
    return pl.pallas_call(
        body,
        grid_spec=pltpu.PrefetchScalarGridSpec(
            num_scalar_prefetch=2,
            grid=(batch,),
            in_specs=[
                pl.BlockSpec((1, span, width), row_index),
                pl.BlockSpec((width, q_width), whole),
                pl.BlockSpec((width, kv_width), whole),
                pl.BlockSpec((width, kv_width), whole),
            ],
            out_specs=[
                pl.BlockSpec((1, span, q_width), lambda t, order, live: (t, 0, 0)),
                pl.BlockSpec(
                    (1, span, 2 * kv_width), lambda t, order, live: (jnp.maximum(t - 1, 0), 0, 0)
                ),
            ],
        ),
        out_shape=[
            jax.ShapeDtypeStruct((batch, span, q_width), jnp.bfloat16),
            jax.ShapeDtypeStruct((batch - 1, span, 2 * kv_width), jnp.bfloat16),
        ],
        cost_estimate=pl.CostEstimate(
            flops=12 * batch * span * width * (q_width + 2 * kv_width) // 4,
            bytes_accessed=8 << 20,
            transcendentals=0,
        ),
        name="other_qkv",
    )(order, live, rows, wq, wk, wv)


def attend_tier(tier, place, order, lengths, flags, spans, extra, bias, queries, own_kv, slabs, wo, parts):
    batch, span, q_width = queries.shape
    blocks = span // KB
    total = bias.shape[2]
    kv_width = own_kv.shape[-1] // 2
    kv_heads = kv_width // HD
    per = q_width // kv_width
    width = wo.shape[1]
    piece = width // (parts * CORES)
    counts = [s.shape[0] for s in slabs]
    scale = HD ** (-0.5) * LOG2E

    def body(place_ref, order_ref, len_ref, flag_ref, span_ref, extra_ref, bias_ref, q_ref, kv_ref, *rest):
        slab_refs = rest[: len(slabs)]
        w_ref, keep_ref, give_ref, top, low, acc, att, mask = rest[len(slabs) :]
        here = place_ref[0]
        seq = order_ref[tier]
        length = len_ref[seq]
        alive = here * span < length

        @pl.when(jnp.logical_not(alive))
        def _():
            keep_ref[...] = jnp.zeros_like(keep_ref)
            give_ref[...] = jnp.zeros_like(give_ref)

        def grouped(head):
            base = head * per * HD
            return jnp.concatenate(
                [q_ref[0, :, base + g * HD : base + (g + 1) * HD] for g in range(per)], axis=0
            )

        def scores(head, keys):
            return lax.dot_general(
                grouped(head), keys, (((1,), (1,)), ((), ())), preferred_element_type=jnp.float32
            )

        @pl.when(alive)
        def _():
            own_bias = bias_ref[0, :, pl.ds(pl.multiple_of(here * span, span), span)]
            key = lax.broadcasted_iota(jnp.int32, (KB, span), 1)
            for i in range(blocks):
                query = i * KB + lax.broadcasted_iota(jnp.int32, (KB, span), 0)
                part = jnp.where(key == query, extra_ref[seq, i], own_bias[i : i + 1])
                mask[i] = jnp.where(key <= query, part, -jnp.inf)
            for head in range(kv_heads):
                s = scores(head, kv_ref[0, :, head * HD : (head + 1) * HD])
                s = (s.reshape(per, blocks, KB, span) + mask[...][None]).reshape(s.shape)
                high = jnp.max(s, axis=-1, keepdims=True)
                e = jnp.exp2((s - high) * scale)
                top[head] = high
                low[head] = jnp.sum(e, axis=-1, keepdims=True)
                acc[head] = jnp.dot(
                    e.astype(jnp.bfloat16),
                    kv_ref[0, :, kv_width + head * HD : kv_width + (head + 1) * HD],
                    preferred_element_type=jnp.float32,
                )

            def take(ref, index, slot):
                source = span_ref[slot]

                @pl.when(jnp.logical_and(source >= 0, flag_ref[seq, jnp.maximum(source, 0)] > 0))
                def _():
                    slab_bias = bias_ref[0, :, pl.ds(pl.multiple_of(source * span, span), span)]
                    for head in range(kv_heads):
                        s = scores(head, ref[index, :, head * HD : (head + 1) * HD])
                        s = s.reshape(per, blocks, KB, span) + slab_bias[None, :, None, :]
                        s = s.reshape(per * span, span)
                        old = top[head]
                        high = jnp.maximum(old, jnp.max(s, axis=-1, keepdims=True))
                        e = jnp.exp2((s - high) * scale)
                        fade = jnp.exp2((old - high) * scale)
                        top[head] = high
                        low[head] = low[head] * fade + jnp.sum(e, axis=-1, keepdims=True)
                        acc[head] = acc[head] * fade + jnp.dot(
                            e.astype(jnp.bfloat16),
                            ref[index, :, kv_width + head * HD : kv_width + (head + 1) * HD],
                            preferred_element_type=jnp.float32,
                        )

            slot = 0
            for ref, count in zip(slab_refs, counts):
                if count == 1:
                    take(ref, 0, slot)
                else:
                    first = slot

                    @pl.loop(0, count)
                    def _(i):
                        take(ref, i, first + i)

                slot += count

            rows = here * span + lax.broadcasted_iota(jnp.int32, (span, 1), 0)
            living = rows < length
            for head in range(kv_heads):
                done = acc[head] / low[head]
                for g in range(per):
                    col = (head * per + g) * HD
                    att[:, col : col + HD] = jnp.where(
                        living, done[g * span : (g + 1) * span], 0.0
                    ).astype(att.dtype)
            mixed = att[...]
            y = place_ref[1]
            core = place_ref[2]
            for out_ref, mine in ((give_ref, CORES - 1 - core), (keep_ref, core)):
                for far in range(parts - 1, -1, -1):
                    column = (lax.rem(y + far, parts) * CORES + mine) * piece
                    out_ref[far] = jnp.dot(
                        mixed,
                        w_ref[:, pl.ds(pl.multiple_of(column, piece), piece)],
                        preferred_element_type=jnp.float32,
                    ).astype(out_ref.dtype)

    slab_specs = [
        pl.BlockSpec(s.shape, lambda i, *_: (0, 0, 0)) for s in slabs
    ]
    own_index = (lambda i, *_: (0, 0, 0)) if tier == 0 else (lambda i, *_: (tier - 1, 0, 0))
    result = jax.ShapeDtypeStruct((parts, span, piece), jnp.bfloat16)
    result_spec = pl.BlockSpec((parts, span, piece), lambda i, *_: (0, 0, 0))
    return pl.pallas_call(
        body,
        grid_spec=pltpu.PrefetchScalarGridSpec(
            num_scalar_prefetch=6,
            grid=(1,),
            in_specs=[
                pl.BlockSpec((1, blocks, total), lambda i, place, order, *_: (order[tier], 0, 0)),
                pl.BlockSpec((1, span, q_width), lambda i, *_: (tier, 0, 0)),
                pl.BlockSpec((1, span, 2 * kv_width), own_index),
                *slab_specs,
                pl.BlockSpec(wo.shape, lambda i, *_: (0, 0)),
            ],
            out_specs=[result_spec, result_spec],
            scratch_shapes=[
                pltpu.VMEM((kv_heads, per * span, 1), jnp.float32),
                pltpu.VMEM((kv_heads, per * span, 1), jnp.float32),
                pltpu.VMEM((kv_heads, per * span, HD), jnp.float32),
                pltpu.VMEM((span, q_width), jnp.bfloat16),
                pltpu.VMEM((blocks, KB, span), jnp.float32),
            ],
        ),
        out_shape=[result, result],
        cost_estimate=pl.CostEstimate(
            flops=6 * span * q_width * width, bytes_accessed=6 << 20, transcendentals=0
        ),
        name=f"attend_{tier}",
    )(place, order, lengths, flags, spans, extra, bias, queries, own_kv, *slabs, wo)


def finish(tier, order, batch, before, keep, got, arrived):
    parts, span, piece = keep.shape

    def body(order_ref, *refs):
        keep_ref, got_ref = refs[0], refs[1]
        arrived_refs = refs[2 : 2 + len(arrived)]
        out_ref = refs[-1]
        total = keep_ref[0].astype(jnp.float32) + got_ref[0].astype(jnp.float32)
        for ref in arrived_refs:
            total = total + ref[...].astype(jnp.float32)
        out_ref[0] = total.astype(out_ref.dtype)

    part_spec = pl.BlockSpec((1, span, piece), lambda i, order: (0, 0, 0))
    flat_spec = pl.BlockSpec((span, piece), lambda i, order: (0, 0))
    in_specs = [part_spec, part_spec] + [flat_spec] * len(arrived)
    operands = [keep, got, *arrived]
    aliases = {}
    if before is not None:
        in_specs.append(pl.BlockSpec(memory_space=pl.ANY))
        operands.append(before)
        aliases = {len(operands): 0}
    return pl.pallas_call(
        body,
        grid_spec=pltpu.PrefetchScalarGridSpec(
            num_scalar_prefetch=1,
            grid=(1,),
            in_specs=in_specs,
            out_specs=pl.BlockSpec((1, span, piece), lambda i, order: (order[tier], 0, 0)),
        ),
        out_shape=jax.ShapeDtypeStruct((batch, span, piece), jnp.bfloat16),
        input_output_aliases=aliases,
        cost_estimate=pl.CostEstimate(
            flops=4 * span * piece, bytes_accessed=8 * span * piece, transcendentals=0
        ),
        name=f"finish_{tier}",
    )(order, *operands)


def gather_spans(slab, reach, columns):
    rows = reach // columns
    arrived = []

    def turn(x, row_from, back):
        for d in range(1, columns):
            pairs = [
                (r * columns + c, r * columns + (c + d) % columns)
                for r in range(row_from, rows)
                for c in range(columns)
                if r > row_from or back > 0 or c + d < columns
            ]
            arrived.append((lax.ppermute(x, "kv", pairs), back, d))

    passing = slab
    hops = []
    for h in range(1, rows):
        pairs = [
            (r * columns + c, (r + 1) * columns + c)
            for r in range(h - 1, rows - 1)
            for c in range(columns)
        ]
        passing = lax.ppermute(passing, "kv", pairs)
        hops.append(passing)
    turn(slab, 0, 0)
    for h, piece in enumerate(hops, start=1):
        arrived.append((piece, h, 0))
        turn(piece, h, h)
    return arrived


def layer(reaches, columns, inputs, wq, wk, wv, wo, chosen, lengths):
    batch, span, width = inputs.shape
    devices = lax.axis_size("kv")
    members = lax.axis_size("tp")
    parts = members // CORES
    here = lax.axis_index("kv").astype(jnp.int32)
    member = lax.axis_index("tp").astype(jnp.int32)
    total = devices * span

    seq = jnp.arange(batch, dtype=jnp.int32)
    ahead = (lengths[None, :] > lengths[:, None]) | (
        (lengths[None, :] == lengths[:, None]) & (seq[None, :] < seq[:, None])
    )
    rank = jnp.sum(ahead.astype(jnp.int32), axis=1)
    order = jnp.sum(jnp.where(rank[None, :] == seq[:, None], seq[None, :], 0), axis=1)
    live = jnp.sum((lengths > here * span).astype(jnp.int32))[None]
    place = jnp.stack([here, member // CORES, member % CORES])

    per_span = span // KB
    key_block = jnp.arange(total, dtype=jnp.int32) // KB
    named = jnp.any(chosen[..., None] == key_block, axis=2)
    bias = jnp.where(named, 0.0, -jnp.inf).astype(jnp.float32)
    span_ids = jnp.arange(devices, dtype=jnp.int32)
    own_block = here * per_span + jnp.arange(per_span, dtype=jnp.int32)
    times = jnp.sum((chosen == own_block[None, :, None]).astype(jnp.float32), axis=2)
    extra = jnp.log2(times) / (HD ** (-0.5) * LOG2E)
    flags = jnp.any(
        (chosen // per_span)[..., None] == span_ids, axis=(1, 2)
    ).astype(jnp.int32)

    kv0 = first_kv(order, inputs, wk, wv)
    queries, kv_rest = other_qkv(order, live, inputs, wq, wk, wv)

    row, column = here // columns, here % columns
    gathered = []
    for tier in range(batch):
        reach = reaches[tier]
        own = kv0 if tier == 0 else kv_rest[tier - 1]
        if reach <= 1:
            gathered.append([])
            continue
        gathered.append(gather_spans(own, reach, columns))

    partner = [(t, t ^ 1) for t in range(members)]
    out = None
    for tier in reversed(range(batch)):
        arrived = gathered[tier]
        reach = max(reaches[tier], 1)
        spans = [jnp.full((), -1, jnp.int32)]
        for _, back, d in arrived:
            source = (row - back) * columns + lax.rem(column - d + columns, columns)
            ok = (source >= 0) & (source < here) & (row - back >= 0) & (here < reach)
            spans.append(jnp.where(ok, source, -1))
        spans = jnp.stack(spans[1:] or spans)
        slabs = [piece[None] for piece, _, _ in arrived]
        if len(slabs) > 8 or reaches[-1] == reaches[0]:
            slabs = [jnp.concatenate(slabs, axis=0)]
        keep, give = attend_tier(
            tier, place, order, lengths, flags, spans, extra, bias, queries,
            kv0[None] if tier == 0 else kv_rest, slabs, wo, parts,
        )
        groups = [
            (k, t) for k in range(reach) for t in range(members)
        ]
        def swap(x, move):
            pairs = [(k * members + t, k * members + move(t)) for k, t in groups]
            return lax.ppermute(x, ("kv", "tp"), pairs)

        got = swap(give, lambda t: t ^ 1)
        coming = []
        for far in range(1, parts):
            both = keep[far].astype(jnp.float32) + got[far].astype(jnp.float32)
            coming.append(
                swap(
                    both.astype(jnp.bfloat16),
                    lambda t, far=far: ((t // CORES + far) % parts) * CORES + t % CORES,
                )
            )
        out = finish(tier, order, batch, out, keep, got, coming)
    return out


def tier_reaches(devices, batch, columns):
    reaches = []
    for tier in range(batch):
        reach = devices >> tier
        if reach > 1:
            reach = -(-reach // columns) * columns
        reaches.append(reach)
    return tuple(reaches)


def solution(mesh):
    placed = (
        P(None, "kv", None),
        P(None, "tp"),
        P(None, "tp"),
        P(None, "tp"),
        P("tp", None),
        P(None, "kv", None),
        P(),
    )
    devices = mesh.shape["kv"]
    columns = 1 << ((devices.bit_length() - 1) // 2)

    def shards(*args):
        batch, span = args[0].shape[0], args[0].shape[1]
        lengths = args[-1]
        common = tier_reaches(devices, batch, columns)
        reach = jnp.array(common, jnp.int32)
        longer = jnp.sum((lengths[None, :] > reach[:, None] * span).astype(jnp.int32), axis=1)
        fits = jnp.all(longer <= jnp.arange(batch, dtype=jnp.int32))
        return lax.cond(
            fits,
            lambda *a: layer(common, columns, *a),
            lambda *a: layer((devices,) * batch, columns, *a),
            *args,
        )

    return jax.shard_map(
        shards, mesh=mesh, in_specs=placed, out_specs=P(None, "kv", "tp"), check_vma=False
    )
```

```python
import math

import jax
import jax.numpy as jnp
from jax import lax
from jax.experimental import pallas as pl
from jax.experimental.pallas import tpu as pltpu
from jax.sharding import PartitionSpec as P

HD = 128
KB = 64
CORES = 2
SCALE = HD ** (-0.5) * math.log2(math.e)


ANY = pl.BlockSpec(memory_space=pl.ANY)
SMEM = pl.BlockSpec(memory_space=pltpu.SMEM)
VMEM = pl.BlockSpec(memory_space=pltpu.VMEM)


def nth_longest(len_ref, tier):
    batch = len_ref.shape[0]
    found = jnp.int32(0)
    for b in range(batch):
        rank = jnp.int32(0)
        for other in range(batch):
            if other < b:
                rank += (len_ref[other] >= len_ref[b]).astype(jnp.int32)
            elif other > b:
                rank += (len_ref[other] > len_ref[b]).astype(jnp.int32)
        found = jnp.where(rank == tier, b, found)
    return found


def cost(flops, moved):
    return pl.CostEstimate(flops=int(flops), bytes_accessed=int(moved), transcendentals=0)


def first_kv(lengths, rows, wk, wv):
    _, span, width = rows.shape
    kv_width = wk.shape[1]
    tiles = 4
    depth = width // tiles

    def body(len_ref, x_ref, k_ref, v_ref, out_ref, x, k, v, acc, sem):
        seq = nth_longest(len_ref, 0)
        alive = lax.axis_index("kv") * span < len_ref[seq]

        @pl.when(alive)
        def _():
            def copies(t):
                part = pl.ds(pl.multiple_of(t * depth, depth), depth)
                return (
                    pltpu.make_async_copy(k_ref.at[part], k.at[t], sem.at[3 * t]),
                    pltpu.make_async_copy(v_ref.at[part], v.at[t], sem.at[3 * t + 1]),
                    pltpu.make_async_copy(x_ref.at[seq, :, part], x.at[t], sem.at[3 * t + 2]),
                )

            for t in range(tiles):
                for copy in copies(t):
                    copy.start()
            acc[...] = jnp.zeros_like(acc)

            @pl.loop(0, tiles)
            def _(t):
                for copy in copies(t):
                    copy.wait()
                acc[:, :kv_width] += jnp.dot(x[t], k[t], preferred_element_type=jnp.float32)
                acc[:, kv_width:] += jnp.dot(x[t], v[t], preferred_element_type=jnp.float32)

            out_ref[...] = acc[...].astype(out_ref.dtype)

    return pl.pallas_call(
        body,
        in_specs=[SMEM, ANY, ANY, ANY],
        out_specs=VMEM,
        out_shape=jax.ShapeDtypeStruct((span, 2 * kv_width), jnp.bfloat16),
        scratch_shapes=[
            pltpu.VMEM((tiles, span, depth), jnp.bfloat16),
            pltpu.VMEM((tiles, depth, kv_width), jnp.bfloat16),
            pltpu.VMEM((tiles, depth, kv_width), jnp.bfloat16),
            pltpu.VMEM((span, 2 * kv_width), jnp.float32),
            pltpu.SemaphoreType.DMA((3 * tiles,)),
        ],
        cost_estimate=cost(4 * span * width * kv_width, 3 << 20),
        name="first_kv",
    )(lengths, rows, wk, wv)


def other_qkv(lengths, rows, wq, wk, wv, after):
    batch, span, width = rows.shape
    kv_width = wk.shape[1]
    q_width = wq.shape[1]

    def body(len_ref, x_ref, q_ref, k_ref, v_ref, _, *rest):
        q_outs, kv_outs = rest[:batch], rest[batch : 2 * batch - 1]
        x, wqs, wks, wvs, q, kv, sem, out_sem = rest[2 * batch - 1 :]
        here = lax.axis_index("kv")
        seqs = [nth_longest(len_ref, tier) for tier in range(batch)]
        alive = [here * span < len_ref[seq] for seq in seqs]
        weights = [
            pltpu.make_async_copy(ref, buf, sem.at[batch + i])
            for i, (ref, buf) in enumerate(((q_ref, wqs), (k_ref, wks), (v_ref, wvs)))
        ]
        inbound = [
            pltpu.make_async_copy(x_ref.at[seqs[tier]], x.at[tier], sem.at[tier])
            for tier in range(batch)
        ]
        q_out = [
            pltpu.make_async_copy(q.at[tier], q_outs[tier], out_sem.at[tier])
            for tier in range(batch)
        ]
        kv_out = [
            pltpu.make_async_copy(kv.at[tier], kv_outs[tier - 1], out_sem.at[batch + tier])
            for tier in range(1, batch)
        ]
        tiers = [*range(1, batch), 0]

        @pl.when(alive[0])
        def _():
            for copy in weights:
                copy.start()
            for tier in tiers:

                @pl.when(alive[tier])
                def _():
                    inbound[tier].start()

            for copy in weights:
                copy.wait()

        @pl.loop(0, batch)
        def _(step):
            tier = lax.rem(step + 1, batch)

            @pl.when(here * span < len_ref[nth_longest(len_ref, tier)])
            def _():
                pltpu.make_async_copy(x_ref.at[0], x.at[tier], sem.at[tier]).wait()
                q[tier] = jnp.dot(
                    x[tier], wqs[...], preferred_element_type=jnp.float32
                ).astype(q.dtype)
                kv[tier, :, :kv_width] = jnp.dot(
                    x[tier], wks[...], preferred_element_type=jnp.float32
                ).astype(kv.dtype)
                kv[tier, :, kv_width:] = jnp.dot(
                    x[tier], wvs[...], preferred_element_type=jnp.float32
                ).astype(kv.dtype)
                for t in range(batch):

                    @pl.when(tier == t)
                    def _():
                        q_out[t].start()
                        if t > 0:
                            kv_out[t - 1].start()

        for tier in tiers:

            @pl.when(alive[tier])
            def _():
                if tier > 0:
                    kv_out[tier - 1].wait()
                q_out[tier].wait()

    outs = pl.pallas_call(
        body,
        in_specs=[SMEM, ANY, ANY, ANY, ANY, ANY],
        out_specs=[ANY] * (2 * batch - 1),
        out_shape=[jax.ShapeDtypeStruct((span, q_width), jnp.bfloat16)] * batch
        + [jax.ShapeDtypeStruct((span, 2 * kv_width), jnp.bfloat16)] * (batch - 1),
        scratch_shapes=[
            pltpu.VMEM((batch, span, width), jnp.bfloat16),
            pltpu.VMEM((width, q_width), jnp.bfloat16),
            pltpu.VMEM((width, kv_width), jnp.bfloat16),
            pltpu.VMEM((width, kv_width), jnp.bfloat16),
            pltpu.VMEM((batch, span, q_width), jnp.bfloat16),
            pltpu.VMEM((batch, span, 2 * kv_width), jnp.bfloat16),
            pltpu.SemaphoreType.DMA((batch + 3,)),
            pltpu.SemaphoreType.DMA((2 * batch,)),
        ],
        cost_estimate=cost(2 * batch * span * width * (q_width + 2 * kv_width), 8 << 20),
        name="other_qkv",
    )(lengths, rows, wq, wk, wv, after)
    return outs[:batch], outs[batch:]


def attend(tiers, columns, lengths, chosen, queries, own_kv, slabs, wo, parts, after=()):
    group = len(tiers)
    span, q_width = queries[0].shape
    blocks = span // KB
    kv_width = own_kv[0].shape[-1] // 2
    kv_heads = kv_width // HD
    per = q_width // kv_width
    width = wo.shape[1]
    piece = width // (parts * CORES)
    names = chosen.shape[2]
    spread = jnp.repeat(jnp.swapaxes(chosen, 1, 2), KB, axis=2)
    devices = lax.axis_size("kv")
    most = max(len(part) for part in slabs)
    room = (most + 1) * blocks
    arrays = [array for part in slabs for array, _, _ in part]

    def body(len_ref, pick_ref, names_ref, *rest):
        q_hbm, kv_hbm = rest[:group], rest[group : 2 * group]
        rest = rest[2 * group :]
        slab_refs = rest[: len(arrays)]
        w_hbm = rest[len(arrays)]
        rest = rest[len(arrays) + 1 + len(after) :]
        keep_hbm, give_hbm, q_ref, w_ref, packed, top, low, acc, att, mask, out = rest[:11]
        marks, listed, count, q_sem, kv_sem, w_sem, slot_sem, out_sem = rest[11:]
        here = lax.axis_index("kv")
        member = lax.axis_index("tp")
        y, core = lax.div(member, CORES), lax.rem(member, CORES)
        row, column = lax.div(here, columns), lax.rem(here, columns)
        load_w = pltpu.make_async_copy(w_hbm, w_ref, w_sem)
        any_alive = here * span < len_ref[nth_longest(len_ref, min(tiers))]

        @pl.when(any_alive)
        def _():
            load_w.start()

        def stores(g, side, far):
            return pltpu.make_async_copy(
                out.at[g, side, far],
                (give_hbm, keep_hbm)[side].at[far, g],
                out_sem.at[g, side, far],
            )

        def one(g, tier):
            seq = nth_longest(len_ref, tier)
            length = len_ref[seq]

            @pl.when(here * span < length)
            def _():
                for i in range(group):

                    @pl.when(g == i)
                    def _():
                        pltpu.make_async_copy(q_hbm[i], q_ref, q_sem).start()
                        pltpu.make_async_copy(
                            kv_hbm[i], packed.at[pl.ds(0, span)], kv_sem
                        ).start()

                for c in range(blocks):
                    listed[c] = here * blocks + c
                count[0] = blocks
                if arrays:

                    @pl.when(here > 0)
                    def _():
                        @pl.loop(0, devices * blocks, unroll=8)
                        def _(b):
                            marks[b] = 0

                        @pl.loop(0, names, unroll=4)
                        def _(t):
                            for i in range(blocks):
                                marks[pick_ref[seq, i, t]] = 1

                    at = 0
                    for i in range(group):
                        for _, back, turned in slabs[i]:
                            ref = slab_refs[at]
                            at += 1
                            source = (row - back) * columns + lax.rem(
                                column - turned + columns, columns
                            )

                            @pl.when((g == i) & (row >= back) & (source < here))
                            def _():
                                @pl.loop(0, blocks)
                                def _(c):
                                    @pl.when(marks[source * blocks + c] > 0)
                                    def _():
                                        slot = count[0]
                                        listed[slot] = source * blocks + c
                                        count[0] = slot + 1
                                        pltpu.make_async_copy(
                                            ref.at[pl.ds(pl.multiple_of(c * KB, KB), KB)],
                                            packed.at[pl.ds(pl.multiple_of(slot * KB, KB), KB)],
                                            slot_sem.at[slot],
                                        ).start()

                picked = names_ref[seq]
                own_id = here * blocks + lax.broadcasted_iota(jnp.int32, (1, span), 1) // KB
                times = jnp.sum((picked == own_id).astype(jnp.float32), axis=0, keepdims=True)
                extra = jnp.log2(times) * (1.0 / SCALE)
                top[...] = jnp.full_like(top, -jnp.inf)
                low[...] = jnp.zeros_like(low)
                acc[...] = jnp.zeros_like(acc)
                pltpu.make_async_copy(q_hbm[0], q_ref, q_sem).wait()
                pltpu.make_async_copy(kv_hbm[0], packed.at[pl.ds(0, span)], kv_sem).wait()
                found = count[0]
                chunks = lax.div(found + blocks - 1, blocks)

                @pl.loop(0, chunks)
                def _(chunk):
                    @pl.when(chunk == 1)
                    def _():
                        @pl.loop(found, chunks * blocks)
                        def _(slot):
                            listed[slot] = -1
                            packed[pl.ds(pl.multiple_of(slot * KB, KB), KB), :] = jnp.zeros(
                                (KB, 2 * kv_width), packed.dtype
                            )

                        @pl.loop(blocks, found)
                        def _(slot):
                            pltpu.make_async_copy(
                                kv_hbm[0].at[pl.ds(0, KB)],
                                packed.at[pl.ds(pl.multiple_of(slot * KB, KB), KB)],
                                slot_sem.at[slot],
                            ).wait()

                    query = lax.broadcasted_iota(jnp.int32, (KB, span), 1)
                    for c in range(blocks):
                        named = picked == listed[chunk * blocks + c]
                        named = jnp.max(jnp.where(named, 0.0, -jnp.inf), axis=0, keepdims=True)
                        key = c * KB + lax.broadcasted_iota(jnp.int32, (KB, span), 0)
                        key = jnp.where(chunk == 0, key, -1)
                        part = jnp.where(key == query, extra, named)
                        mask[c] = jnp.where(key <= query, part, -jnp.inf)
                    at = pl.ds(pl.multiple_of(chunk * span, span), span)
                    for head in range(kv_heads):
                        base = head * per * HD
                        rows = jnp.concatenate(
                            [q_ref[:, base + k * HD : base + (k + 1) * HD] for k in range(per)],
                            axis=0,
                        )
                        s = lax.dot_general(
                            packed[at, head * HD : (head + 1) * HD],
                            rows,
                            (((1,), (1,)), ((), ())),
                            preferred_element_type=jnp.float32,
                        )
                        bias = mask[...].reshape(span, span)
                        s = s + jnp.concatenate([bias] * per, axis=1)
                        old = top[head]
                        high = jnp.maximum(old, jnp.max(s, axis=0, keepdims=True))
                        e = jnp.exp2((s - high) * SCALE)
                        fade = jnp.exp2((old - high) * SCALE)
                        top[head] = high
                        low[head] = low[head] * fade + jnp.sum(e, axis=0, keepdims=True)
                        acc[head] = acc[head] * fade + lax.dot_general(
                            packed[at, kv_width + head * HD : kv_width + (head + 1) * HD],
                            e.astype(jnp.bfloat16),
                            (((0,), (0,)), ((), ())),
                            preferred_element_type=jnp.float32,
                        )

                living = here * span + lax.broadcasted_iota(jnp.int32, (span, 1), 0) < length
                for head in range(kv_heads):
                    done = acc[head] * (1.0 / low[head])
                    for k in range(per):
                        col = (head * per + k) * HD
                        att[:, col : col + HD] = jnp.where(
                            living, done[:, k * span : (k + 1) * span].T, 0.0
                        ).astype(att.dtype)

                @pl.when((g == 0) | (here * span >= len_ref[nth_longest(len_ref, tier + 1)]))
                def _():
                    load_w.wait()

                for side in range(CORES):
                    mine = (CORES - 1 - core, core)[side]

                    @pl.loop(0, parts)
                    def _(step):
                        far = parts - 1 - step
                        first = (lax.rem(y + far, parts) * CORES + mine) * piece
                        out[g, side, far] = jnp.dot(
                            att[...],
                            w_ref[:, pl.ds(pl.multiple_of(first, piece), piece)],
                            preferred_element_type=jnp.float32,
                        ).astype(out.dtype)
                        stores(g, side, far).start()

        if group == 1:
            one(0, tiers[0])
        else:

            @pl.loop(0, group)
            def _(g):
                one(g, tiers[0] - g)

        for g in range(group):

            @pl.when(here * span < len_ref[nth_longest(len_ref, tiers[g])])
            def _():
                for side in range(CORES):
                    for far in range(parts):
                        stores(g, side, far).wait()

    result = jax.ShapeDtypeStruct((parts, group, span, piece), jnp.bfloat16)
    return pl.pallas_call(
        body,
        in_specs=[SMEM, SMEM, VMEM, *[ANY] * (2 * group + len(arrays) + 1 + len(after))],
        out_specs=[ANY, ANY],
        out_shape=[result, result],
        scratch_shapes=[
            pltpu.VMEM((span, q_width), jnp.bfloat16),
            pltpu.VMEM(wo.shape, jnp.bfloat16),
            pltpu.VMEM((room * KB, 2 * kv_width), jnp.bfloat16),
            pltpu.VMEM((kv_heads, 1, per * span), jnp.float32),
            pltpu.VMEM((kv_heads, 1, per * span), jnp.float32),
            pltpu.VMEM((kv_heads, HD, per * span), jnp.float32),
            pltpu.VMEM((span, q_width), jnp.bfloat16),
            pltpu.VMEM((blocks, KB, span), jnp.float32),
            pltpu.VMEM((group, CORES, parts, span, piece), jnp.bfloat16),
            pltpu.SMEM((devices * blocks,), jnp.int32),
            pltpu.SMEM((room,), jnp.int32),
            pltpu.SMEM((1,), jnp.int32),
            pltpu.SemaphoreType.DMA,
            pltpu.SemaphoreType.DMA,
            pltpu.SemaphoreType.DMA,
            pltpu.SemaphoreType.DMA((room,)),
            pltpu.SemaphoreType.DMA((group, CORES, parts)),
        ],
        cost_estimate=cost(group * 4 * span * q_width * width, group * (3 << 20)),
    )(lengths, chosen, spread, *queries, *own_kv, *arrays, wo, *after)


def finish(lengths, batch, groups):
    _, _, span, piece = groups[0][1].shape

    def body(len_ref, *refs):
        out_ref = refs[-1]
        at = 0
        for tiers, _, _, coming in groups:
            mine = refs[at : at + 2 + len(coming)]
            at += 2 + len(coming)
            for g, tier in enumerate(tiers):
                seq = nth_longest(len_ref, tier)
                alive = lax.axis_index("kv") * span < len_ref[seq]

                @pl.when(alive)
                def _():
                    total = mine[0][0, g].astype(jnp.float32) + mine[1][0, g].astype(jnp.float32)
                    for ref in mine[2:]:
                        total = total + ref[g].astype(jnp.float32)
                    out_ref[seq] = total.astype(out_ref.dtype)

                @pl.when(jnp.logical_not(alive))
                def _():
                    out_ref[seq] = jnp.zeros((span, piece), out_ref.dtype)

    specs, operands = [SMEM], [lengths]
    for tiers, keep, got, coming in groups:
        size = len(tiers)
        near = pl.BlockSpec((1, size, span, piece), lambda i: (0, 0, 0, 0))
        flat = pl.BlockSpec((size, span, piece), lambda i: (0, 0, 0))
        specs += [near, near] + [flat] * len(coming)
        operands += [keep, got, *coming]
    return pl.pallas_call(
        body,
        grid=(1,),
        in_specs=specs,
        out_specs=pl.BlockSpec((batch, span, piece), lambda i: (0, 0, 0)),
        out_shape=jax.ShapeDtypeStruct((batch, span, piece), jnp.bfloat16),
        cost_estimate=cost(batch * 4 * span * piece, batch * 8 * span * piece),
        name="finish",
    )(*operands)


def gather_spans(slab, reach, columns):
    rows = reach // columns
    arrived = []

    def turn(x, back):
        for d in range(1, columns):
            pairs = [
                (r * columns + c, r * columns + (c + d) % columns)
                for r in range(back, rows)
                for c in range(columns)
                if r > 0 or c + d < columns
            ]
            arrived.append((lax.ppermute(x, "kv", pairs), back, d))

    turn(slab, 0)
    passing = slab
    for back in range(1, rows):
        pairs = [
            (r * columns + c, (r + 1) * columns + c)
            for r in range(back - 1, rows - 1)
            for c in range(columns)
        ]
        passing = lax.ppermute(passing, "kv", pairs)
        arrived.append((passing, back, 0))
        turn(passing, back)
    return arrived


def layer(reaches, together, columns, inputs, wq, wk, wv, wo, chosen, lengths):
    batch, _, _ = inputs.shape
    members = lax.axis_size("tp")
    parts = members // CORES

    kv0 = first_kv(lengths, inputs, wk, wv)
    queries, kv_rest = other_qkv(lengths, inputs, wq, wk, wv, kv0)
    own = [kv0, *kv_rest]
    gathered = [
        gather_spans(own[tier], reaches[tier], columns) if reaches[tier] > 1 else []
        for tier in range(batch)
    ]

    groups = []
    for tiers in together:
        reach = max(max(reaches[tier] for tier in tiers), 1)
        keep, give = attend(
            tiers,
            columns,
            lengths,
            chosen,
            [queries[tier] for tier in tiers],
            [own[tier] for tier in tiers],
            [gathered[tier] for tier in tiers],
            wo,
            parts,
        )

        def swap(x, move):
            pairs = [
                (k * members + t, k * members + move(t))
                for k in range(reach)
                for t in range(members)
            ]
            return lax.ppermute(x, ("kv", "tp"), pairs)

        got = swap(give, lambda t: t ^ 1)
        coming = []
        for far in range(1, parts):
            both = keep[far].astype(jnp.float32) + got[far].astype(jnp.float32)
            coming.append(
                swap(
                    both.astype(jnp.bfloat16),
                    lambda t, far=far: ((t // CORES + far) % parts) * CORES + t % CORES,
                )
            )
        groups.append((tiers, keep, got, coming))
    return finish(lengths, batch, groups)


def tier_reaches(devices, batch, columns):
    reaches = []
    for tier in range(batch):
        reach = devices >> tier
        if reach > 1:
            reach = -(-reach // columns) * columns
        reaches.append(reach)
    return tuple(reaches)


def solution(mesh):
    placed = (
        P(None, "kv", None),
        P(None, "tp"),
        P(None, "tp"),
        P(None, "tp"),
        P("tp", None),
        P(None, "kv", None),
        P(),
    )
    devices = mesh.shape["kv"]
    columns = 1 << ((devices.bit_length() - 1) // 2)

    def shards(*args):
        batch, span = args[0].shape[0], args[0].shape[1]
        lengths = args[-1]
        common = tier_reaches(devices, batch, columns)
        backwards = range(batch - 1, -1, -1)
        together = (tuple(backwards[:2]), *((tier,) for tier in backwards[2:]))
        out = layer(common, together, columns, *args)
        reach = jnp.array(common, jnp.int32)
        longer = jnp.sum((lengths[None, :] > reach[:, None] * span).astype(jnp.int32), axis=1)
        fits = jnp.all(longer <= jnp.arange(batch, dtype=jnp.int32))
        return lax.cond(
            fits,
            lambda done, *a: done,
            lambda done, *a: layer((devices,) * batch, (tuple(backwards),), columns, *a),
            out,
            *args,
        )

    return jax.shard_map(
        shards, mesh=mesh, in_specs=placed, out_specs=P(None, "kv", "tp"), check_vma=False
    )
```

```python
import math

import jax
import jax.numpy as jnp
from jax import lax
from jax.experimental import pallas as pl
from jax.experimental.pallas import tpu as pltpu
from jax.sharding import PartitionSpec as P

HD = 128
KB = 64
CORES = 2
ROOM = 24 << 20
SCALE = HD ** (-0.5) * math.log2(math.e)


ANY = pl.BlockSpec(memory_space=pl.ANY)
SMEM = pl.BlockSpec(memory_space=pltpu.SMEM)
VMEM = pl.BlockSpec(memory_space=pltpu.VMEM)


def nth_longest(len_ref, tier):
    batch = len_ref.shape[0]
    found = jnp.int32(0)
    for b in range(batch):
        rank = jnp.int32(0)
        for other in range(batch):
            if other < b:
                rank += (len_ref[other] >= len_ref[b]).astype(jnp.int32)
            elif other > b:
                rank += (len_ref[other] > len_ref[b]).astype(jnp.int32)
        found = jnp.where(rank == tier, b, found)
    return found


def cost(flops, moved):
    return pl.CostEstimate(flops=int(flops), bytes_accessed=int(moved), transcendentals=0)


def project(lengths, rows, weights, first=0, shared=0, after=()):
    batch, span, width = rows.shape
    sets = len(weights)
    widths = [sum(w.shape[1] for w in part) for part in weights]
    flat = [w for part in weights for w in part]
    more = min(shared, 1)

    def body(len_ref, x_ref, *refs):
        given, refs = refs[: len(flat)], refs[len(flat) + len(after) :]
        outs, refs = refs[: sets * batch], refs[sets * batch :]
        again, refs = refs[:more], refs[more:]
        x, refs = refs[0], refs[1:]
        held, out, (sem, w_sem, out_sem) = refs[:sets], refs[sets : 2 * sets], refs[2 * sets :]
        here = lax.axis_index("kv")
        seqs = [nth_longest(len_ref, tier) for tier in range(batch)]
        alive = [here * span < len_ref[seq] for seq in seqs]
        loads, at = [], 0
        for i, part in enumerate(weights):
            loads.append([])
            base = 0
            for w in part:
                loads[i].append(
                    pltpu.make_async_copy(
                        given[at], held[i].at[:, pl.ds(base, w.shape[1])], w_sem.at[at]
                    )
                )
                at += 1
                base += w.shape[1]

        def load(tier):
            return pltpu.make_async_copy(x_ref.at[seqs[tier]], x.at[tier], sem.at[tier])

        def stores(tier):
            found = [
                pltpu.make_async_copy(
                    out[i].at[tier], outs[i * batch + tier], out_sem.at[i, tier]
                )
                for i in range(sets)
            ]
            if first <= tier < first + shared:
                found.append(
                    pltpu.make_async_copy(
                        out[0].at[tier], again[0].at[tier - first], out_sem.at[sets, tier]
                    )
                )
            return found

        @pl.when(alive[0])
        def _():
            load(0).start()
            for part in loads:
                for one in part:
                    one.start()

        for tier in range(1, batch):

            @pl.when(alive[tier])
            def _():
                load(tier).start()

        @pl.loop(0, batch)
        def _(tier):
            @pl.when(here * span < len_ref[nth_longest(len_ref, tier)])
            def _():
                pltpu.make_async_copy(x_ref.at[0], x.at[tier], sem.at[tier]).wait()
                for i in range(sets):

                    @pl.when(tier == 0)
                    def _():
                        for one in loads[i]:
                            one.wait()

                    out[i][tier] = jnp.dot(
                        x[tier], held[i][...], preferred_element_type=jnp.float32
                    ).astype(out[i].dtype)
                for t in range(batch):

                    @pl.when(tier == t)
                    def _():
                        for store in stores(t):
                            store.start()

        for tier in range(batch):

            @pl.when(alive[tier])
            def _():
                for store in stores(tier):
                    store.wait()

    found = pl.pallas_call(
        body,
        in_specs=[SMEM] + [ANY] * (1 + len(flat) + len(after)),
        out_specs=[ANY] * (sets * batch + more),
        out_shape=[
            jax.ShapeDtypeStruct((span, size), jnp.bfloat16) for size in widths for _ in range(batch)
        ]
        + [jax.ShapeDtypeStruct((shared, span, widths[0]), jnp.bfloat16)] * more,
        scratch_shapes=[pltpu.VMEM((batch, span, width), jnp.bfloat16)]
        + [pltpu.VMEM((width, size), jnp.bfloat16) for size in widths]
        + [pltpu.VMEM((batch, span, size), jnp.bfloat16) for size in widths]
        + [
            pltpu.SemaphoreType.DMA((batch,)),
            pltpu.SemaphoreType.DMA((len(flat),)),
            pltpu.SemaphoreType.DMA((sets + 1, batch)),
        ],
        compiler_params=pltpu.CompilerParams(vmem_limit_bytes=ROOM),
        cost_estimate=cost(2 * batch * span * width * sum(widths), 8 << 20),
    )(lengths, rows, *flat, *after)
    return [found[i * batch : (i + 1) * batch] for i in range(sets)], found[-1]


def attend(tiers, columns, lengths, chosen, queries, own_kv, slabs, wo, parts):
    group = len(tiers)
    span, q_width = queries[0].shape
    blocks = span // KB
    kv_width = own_kv[0].shape[-1] // 2
    kv_heads = kv_width // HD
    per = q_width // kv_width
    width = wo.shape[1]
    piece = width // (parts * CORES)
    names = chosen.shape[2]
    devices = lax.axis_size("kv")
    most = max(len(part) for part in slabs)
    room = (most + 1) * blocks
    arrays = [array for part in slabs for array, _, _, _ in part]

    def body(len_ref, pick_ref, names_ref, *rest):
        q_hbm, kv_hbm = rest[:group], rest[group : 2 * group]
        rest = rest[2 * group :]
        slab_refs = rest[: len(arrays)]
        w_hbm = rest[len(arrays)]
        rest = rest[len(arrays) + 1 :]
        keep_hbm, give_hbm, q_ref, w_ref, packed, top, low, acc, att, mask, out = rest[:11]
        marks, listed, count, q_sem, kv_sem, w_sem, slot_sem, out_sem = rest[11:]
        here = lax.axis_index("kv")
        member = lax.axis_index("tp")
        y, core = lax.div(member, CORES), lax.rem(member, CORES)
        row, column = lax.div(here, columns), lax.rem(here, columns)
        load_w = pltpu.make_async_copy(w_hbm, w_ref, w_sem)
        any_alive = here * span < len_ref[nth_longest(len_ref, min(tiers))]

        @pl.when(any_alive)
        def _():
            load_w.start()

        def stores(g, side, far):
            return pltpu.make_async_copy(
                out.at[g, side, far],
                (give_hbm, keep_hbm)[side].at[far, g],
                out_sem.at[g, side, far],
            )

        def load(g):
            for i in range(group):

                @pl.when(g == i)
                def _():
                    pltpu.make_async_copy(q_hbm[i], q_ref, q_sem).start()
                    pltpu.make_async_copy(kv_hbm[i], packed.at[pl.ds(0, span)], kv_sem).start()

        def one(g, tier):
            seq = nth_longest(len_ref, tier)
            length = len_ref[seq]

            @pl.when(here * span < length)
            def _():
                opening = (g == 0) | (here * span >= len_ref[nth_longest(len_ref, tier + 1)])

                @pl.when(opening)
                def _():
                    load(g)

                for c in range(blocks):
                    listed[c] = here * blocks + c
                count[0] = blocks
                if arrays:

                    @pl.when(here > 0)
                    def _():
                        @pl.loop(0, devices * blocks, unroll=8)
                        def _(b):
                            marks[b] = 0

                        @pl.loop(0, names, unroll=4)
                        def _(t):
                            for i in range(blocks):
                                marks[pick_ref[seq, i, t]] = 1

                    at = 0
                    for i in range(group):
                        for _, place, back, turned in slabs[i]:
                            ref = slab_refs[at] if place is None else slab_refs[at].at[place]
                            at += 1
                            source = (row - back) * columns + lax.rem(
                                column - turned + columns, columns
                            )

                            @pl.when((g == i) & (row >= back) & (source < here))
                            def _():
                                @pl.loop(0, blocks)
                                def _(c):
                                    @pl.when(marks[source * blocks + c] > 0)
                                    def _():
                                        slot = count[0]
                                        listed[slot] = source * blocks + c
                                        count[0] = slot + 1
                                        pltpu.make_async_copy(
                                            ref.at[pl.ds(pl.multiple_of(c * KB, KB), KB)],
                                            packed.at[pl.ds(pl.multiple_of(slot * KB, KB), KB)],
                                            slot_sem.at[slot],
                                        ).start()

                widen = lax.broadcasted_iota(jnp.int32, (blocks, span), 1) // KB
                widen = widen == lax.broadcasted_iota(jnp.int32, (blocks, span), 0)
                picked = lax.dot_general(
                    names_ref[seq].astype(jnp.float32),
                    widen.astype(jnp.float32),
                    (((0,), (0,)), ((), ())),
                    precision=lax.Precision.HIGHEST,
                    preferred_element_type=jnp.float32,
                )
                picked = jnp.round(picked).astype(jnp.int32)
                own_id = here * blocks + lax.broadcasted_iota(jnp.int32, (1, span), 1) // KB
                times = jnp.sum((picked == own_id).astype(jnp.float32), axis=0, keepdims=True)
                extra = jnp.log2(times) * (1.0 / SCALE)
                top[...] = jnp.full_like(top, -jnp.inf)
                low[...] = jnp.zeros_like(low)
                acc[...] = jnp.zeros_like(acc)
                pltpu.make_async_copy(q_hbm[0], q_ref, q_sem).wait()
                pltpu.make_async_copy(kv_hbm[0], packed.at[pl.ds(0, span)], kv_sem).wait()
                found = count[0]
                chunks = lax.div(found + blocks - 1, blocks)

                @pl.loop(0, chunks)
                def _(chunk):
                    @pl.when(chunk == 1)
                    def _():
                        @pl.loop(found, chunks * blocks)
                        def _(slot):
                            listed[slot] = -1
                            packed[pl.ds(pl.multiple_of(slot * KB, KB), KB), :] = jnp.zeros(
                                (KB, 2 * kv_width), packed.dtype
                            )

                        @pl.loop(blocks, found)
                        def _(slot):
                            pltpu.make_async_copy(
                                kv_hbm[0].at[pl.ds(0, KB)],
                                packed.at[pl.ds(pl.multiple_of(slot * KB, KB), KB)],
                                slot_sem.at[slot],
                            ).wait()

                    query = lax.broadcasted_iota(jnp.int32, (KB, span), 1)
                    for c in range(blocks):
                        named = picked == listed[chunk * blocks + c]
                        named = jnp.max(jnp.where(named, 0.0, -jnp.inf), axis=0, keepdims=True)
                        key = c * KB + lax.broadcasted_iota(jnp.int32, (KB, span), 0)
                        key = jnp.where(chunk == 0, key, -1)
                        part = jnp.where(key == query, extra, named)
                        mask[c] = jnp.where(key <= query, part, -jnp.inf)
                    at = pl.ds(pl.multiple_of(chunk * span, span), span)
                    for head in range(kv_heads):
                        base = head * per * HD
                        rows = jnp.concatenate(
                            [q_ref[:, base + k * HD : base + (k + 1) * HD] for k in range(per)],
                            axis=0,
                        )
                        s = lax.dot_general(
                            packed[at, head * HD : (head + 1) * HD],
                            rows,
                            (((1,), (1,)), ((), ())),
                            preferred_element_type=jnp.float32,
                        )
                        bias = mask[...].reshape(span, span)
                        s = s + jnp.concatenate([bias] * per, axis=1)
                        old = top[head]
                        high = jnp.maximum(old, jnp.max(s, axis=0, keepdims=True))
                        e = jnp.exp2((s - high) * SCALE)
                        fade = jnp.exp2((old - high) * SCALE)
                        top[head] = high
                        low[head] = low[head] * fade + jnp.sum(e, axis=0, keepdims=True)
                        acc[head] = acc[head] * fade + lax.dot_general(
                            packed[at, kv_width + head * HD : kv_width + (head + 1) * HD],
                            e.astype(jnp.bfloat16),
                            (((0,), (0,)), ((), ())),
                            preferred_element_type=jnp.float32,
                        )

                load(g + 1)
                living = here * span + lax.broadcasted_iota(jnp.int32, (span, 1), 0) < length
                for head in range(kv_heads):
                    done = acc[head] * (1.0 / low[head])
                    for k in range(per):
                        col = (head * per + k) * HD
                        att[:, col : col + HD] = jnp.where(
                            living, done[:, k * span : (k + 1) * span].T, 0.0
                        ).astype(att.dtype)

                @pl.when(opening)
                def _():
                    load_w.wait()

                for side in range(CORES):
                    mine = (CORES - 1 - core, core)[side]

                    @pl.loop(0, parts)
                    def _(step):
                        far = parts - 1 - step
                        first = (lax.rem(y + far, parts) * CORES + mine) * piece
                        out[g, side, far] = jnp.dot(
                            att[...],
                            w_ref[:, pl.ds(pl.multiple_of(first, piece), piece)],
                            preferred_element_type=jnp.float32,
                        ).astype(out.dtype)
                        stores(g, side, far).start()

        if group == 1:
            one(0, tiers[0])
        else:

            @pl.loop(0, group)
            def _(g):
                one(g, tiers[0] - g)

        for g in range(group):

            @pl.when(here * span < len_ref[nth_longest(len_ref, tiers[g])])
            def _():
                for side in range(CORES):
                    for far in range(parts):
                        stores(g, side, far).wait()

    result = jax.ShapeDtypeStruct((parts, group, span, piece), jnp.bfloat16)
    return pl.pallas_call(
        body,
        in_specs=[SMEM, SMEM, VMEM, *[ANY] * (2 * group + len(arrays) + 1)],
        out_specs=[ANY, ANY],
        out_shape=[result, result],
        scratch_shapes=[
            pltpu.VMEM((span, q_width), jnp.bfloat16),
            pltpu.VMEM(wo.shape, jnp.bfloat16),
            pltpu.VMEM((room * KB, 2 * kv_width), jnp.bfloat16),
            pltpu.VMEM((kv_heads, 1, per * span), jnp.float32),
            pltpu.VMEM((kv_heads, 1, per * span), jnp.float32),
            pltpu.VMEM((kv_heads, HD, per * span), jnp.float32),
            pltpu.VMEM((span, q_width), jnp.bfloat16),
            pltpu.VMEM((blocks, KB, span), jnp.float32),
            pltpu.VMEM((group, CORES, parts, span, piece), jnp.bfloat16),
            pltpu.SMEM((devices * blocks,), jnp.int32),
            pltpu.SMEM((room,), jnp.int32),
            pltpu.SMEM((1,), jnp.int32),
            pltpu.SemaphoreType.DMA,
            pltpu.SemaphoreType.DMA,
            pltpu.SemaphoreType.DMA,
            pltpu.SemaphoreType.DMA((room,)),
            pltpu.SemaphoreType.DMA((group, CORES, parts)),
        ],
        compiler_params=pltpu.CompilerParams(vmem_limit_bytes=ROOM),
        cost_estimate=cost(group * 4 * span * q_width * width, group * (3 << 20)),
    )(lengths, chosen, chosen, *queries, *own_kv, *arrays, wo)


def finish(lengths, batch, groups, before=None):
    parts, _, span, piece = groups[0][1].shape
    every = [(tier, g, at) for at, group in enumerate(groups) for g, tier in enumerate(group[0])]
    each = 1 + parts

    def body(len_ref, *refs):
        given = refs[: each * len(groups)]
        out_ref, terms, sums, in_sem, out_sem = refs[-5:]
        here = lax.axis_index("kv")
        seqs = [nth_longest(len_ref, tier) for tier, _, _ in every]

        def loads(n):
            _, g, at = every[n]
            mine = given[at * each : (at + 1) * each]
            sources = [mine[0].at[0, g], mine[1].at[0, g]] + [ref.at[g] for ref in mine[2:]]
            return [
                pltpu.make_async_copy(source, terms.at[n, i], in_sem.at[n, i])
                for i, source in enumerate(sources)
            ]

        def store(n):
            return pltpu.make_async_copy(sums.at[n], out_ref.at[seqs[n]], out_sem.at[n])

        for n in range(len(every)):

            @pl.when(here * span < len_ref[seqs[n]])
            def _():
                for load in loads(n):
                    load.start()

        for n in range(len(every)):
            alive = here * span < len_ref[seqs[n]]

            @pl.when(alive)
            def _():
                for load in loads(n):
                    load.wait()
                total = terms[n, 0].astype(jnp.float32)
                for i in range(1, each):
                    total = total + terms[n, i].astype(jnp.float32)
                sums[n] = total.astype(sums.dtype)

            @pl.when(jnp.logical_not(alive))
            def _():
                sums[n] = jnp.zeros((span, piece), sums.dtype)

            store(n).start()
        for n in range(len(every)):
            store(n).wait()

    operands = [part for _, keep, got, coming in groups for part in (keep, got, *coming)]
    aliases = {}
    if before is not None:
        aliases = {1 + len(operands): 0}
        operands.append(before)
    return pl.pallas_call(
        body,
        in_specs=[SMEM] + [ANY] * len(operands),
        out_specs=ANY,
        out_shape=jax.ShapeDtypeStruct((batch, span, piece), jnp.bfloat16),
        scratch_shapes=[
            pltpu.VMEM((len(every), each, span, piece), jnp.bfloat16),
            pltpu.VMEM((len(every), span, piece), jnp.bfloat16),
            pltpu.SemaphoreType.DMA((len(every), each)),
            pltpu.SemaphoreType.DMA((len(every),)),
        ],
        input_output_aliases=aliases,
        compiler_params=pltpu.CompilerParams(vmem_limit_bytes=ROOM),
        cost_estimate=cost(len(every) * 4 * span * piece, len(every) * 8 * span * piece),
        name="finish",
    )(lengths, *operands)


def gather_spans(slabs, joined, first, reaches, columns):
    arrived = [[] for _ in reaches]

    def turn(x, back, rows):
        found = []
        for d in range(1, columns):
            pairs = [
                (r * columns + c, r * columns + (c + d) % columns)
                for r in range(back, rows)
                for c in range(columns)
                if r > 0 or c + d < columns
            ]
            found.append((lax.ppermute(x, "kv", pairs), d))
        return found

    for moved, d in turn(joined, 0, reaches[first] // columns):
        for place in range(joined.shape[0]):
            arrived[first + place].append((moved, place, 0, d))
    for tier, reach in enumerate(reaches):
        rows = reach // columns
        if reach > 1 and not first <= tier < first + joined.shape[0]:
            for moved, d in turn(slabs[tier], 0, rows):
                arrived[tier].append((moved, None, 0, d))
        passing = slabs[tier]
        for back in range(1, rows):
            pairs = [
                (r * columns + c, (r + 1) * columns + c)
                for r in range(back - 1, rows - 1)
                for c in range(columns)
            ]
            passing = lax.ppermute(passing, "kv", pairs)
            arrived[tier].append((passing, None, back, 0))
            for moved, d in turn(passing, back, rows):
                arrived[tier].append((moved, None, back, d))
    return arrived


def layer(reaches, together, columns, inputs, wq, wk, wv, wo, chosen, lengths):
    batch, _, _ = inputs.shape
    members = lax.axis_size("tp")
    parts = members // CORES

    first = 1
    shared = sum(reach > 1 for reach in reaches) - first
    (own, queries), joined = project(lengths, inputs, ((wk, wv), (wq,)), first, shared)
    gathered = gather_spans(own, joined, first, reaches, columns)

    groups = []
    for tiers in together:
        reach = max(max(reaches[tier] for tier in tiers), 1)
        keep, give = attend(
            tiers,
            columns,
            lengths,
            chosen,
            [queries[tier] for tier in tiers],
            [own[tier] for tier in tiers],
            [gathered[tier] for tier in tiers],
            wo,
            parts,
        )

        def swap(x, move):
            pairs = [
                (k * members + t, k * members + move(t))
                for k in range(reach)
                for t in range(members)
            ]
            return lax.ppermute(x, ("kv", "tp"), pairs)

        got = swap(give, lambda t: t ^ 1)
        coming = []
        for far in range(1, parts):
            both = keep[far].astype(jnp.float32) + got[far].astype(jnp.float32)
            coming.append(
                swap(
                    both.astype(jnp.bfloat16),
                    lambda t, far=far: ((t // CORES + far) % parts) * CORES + t % CORES,
                )
            )
        groups.append((tiers, keep, got, coming))
    out = None
    if len(groups) > 1:
        out = finish(lengths, batch, groups[:-1])
    return finish(lengths, batch, groups[-1:], out)


def tier_reaches(devices, batch, columns):
    reaches = []
    for tier in range(batch):
        reach = devices >> tier
        if reach > 1:
            reach = -(-reach // columns) * columns
        reaches.append(reach)
    return tuple(reaches)


def solution(mesh):
    placed = (
        P(None, "kv", None),
        P(None, "tp"),
        P(None, "tp"),
        P(None, "tp"),
        P("tp", None),
        P(None, "kv", None),
        P(),
    )
    devices = mesh.shape["kv"]
    columns = 1 << ((devices.bit_length() - 1) // 2)

    def shards(*args):
        batch, span = args[0].shape[0], args[0].shape[1]
        lengths = args[-1]
        common = tier_reaches(devices, batch, columns)
        backwards = range(batch - 1, -1, -1)
        together = (tuple(backwards[:1]), tuple(backwards[1:-1]), tuple(backwards[-1:]))
        out = layer(common, together, columns, *args)
        reach = jnp.array(common, jnp.int32)
        longer = jnp.sum((lengths[None, :] > reach[:, None] * span).astype(jnp.int32), axis=1)
        fits = jnp.all(longer <= jnp.arange(batch, dtype=jnp.int32))
        return lax.cond(
            fits,
            lambda done, *a: done,
            lambda done, *a: layer((devices,) * batch, (tuple(backwards),), columns, *a),
            out,
            *args,
        )

    return jax.shard_map(
        shards, mesh=mesh, in_specs=placed, out_specs=P(None, "kv", "tp"), check_vma=False
    )
```

```python
import math

import jax
import jax.numpy as jnp
from jax import lax
from jax.experimental import pallas as pl
from jax.experimental.pallas import tpu as pltpu
from jax.sharding import PartitionSpec as P

HD = 128
KB = 64
CORES = 2
ROOM = 24 << 20
SCALE = HD ** (-0.5) * math.log2(math.e)


ANY = pl.BlockSpec(memory_space=pl.ANY)
SMEM = pl.BlockSpec(memory_space=pltpu.SMEM)
VMEM = pl.BlockSpec(memory_space=pltpu.VMEM)


def nth_longest(len_ref, tier):
    batch = len_ref.shape[0]
    found = jnp.int32(0)
    for b in range(batch):
        rank = jnp.int32(0)
        for other in range(batch):
            if other < b:
                rank += (len_ref[other] >= len_ref[b]).astype(jnp.int32)
            elif other > b:
                rank += (len_ref[other] > len_ref[b]).astype(jnp.int32)
        found = jnp.where(rank == tier, b, found)
    return found


def cost(flops, moved):
    return pl.CostEstimate(flops=int(flops), bytes_accessed=int(moved), transcendentals=0)


def project(lengths, rows, weights, first=0, shared=0, after=()):
    batch, span, width = rows.shape
    sets = len(weights)
    widths = [sum(w.shape[1] for w in part) for part in weights]
    flat = [w for part in weights for w in part]
    more = min(shared, 1)

    def body(len_ref, x_ref, *refs):
        given, refs = refs[: len(flat)], refs[len(flat) + len(after) :]
        outs, refs = refs[: sets * batch], refs[sets * batch :]
        again, refs = refs[:more], refs[more:]
        x, refs = refs[0], refs[1:]
        held, out, (sem, w_sem, out_sem) = refs[:sets], refs[sets : 2 * sets], refs[2 * sets :]
        here = lax.axis_index("kv")
        seqs = [nth_longest(len_ref, tier) for tier in range(batch)]
        alive = [here * span < len_ref[seq] for seq in seqs]
        loads, at = [], 0
        for i, part in enumerate(weights):
            loads.append([])
            base = 0
            for w in part:
                loads[i].append(
                    pltpu.make_async_copy(
                        given[at], held[i].at[:, pl.ds(base, w.shape[1])], w_sem.at[at]
                    )
                )
                at += 1
                base += w.shape[1]

        def load(tier):
            return pltpu.make_async_copy(x_ref.at[seqs[tier]], x.at[tier], sem.at[tier])

        def stores(tier):
            found = [
                pltpu.make_async_copy(
                    out[i].at[tier], outs[i * batch + tier], out_sem.at[i, tier]
                )
                for i in range(sets)
            ]
            if first <= tier < first + shared:
                found.append(
                    pltpu.make_async_copy(
                        out[0].at[tier], again[0].at[tier - first], out_sem.at[sets, tier]
                    )
                )
            return found

        @pl.when(alive[0])
        def _():
            load(0).start()
            for part in loads:
                for one in part:
                    one.start()

        for tier in range(1, batch):

            @pl.when(alive[tier])
            def _():
                load(tier).start()

        @pl.loop(0, batch)
        def _(tier):
            @pl.when(here * span < len_ref[nth_longest(len_ref, tier)])
            def _():
                pltpu.make_async_copy(x_ref.at[0], x.at[tier], sem.at[tier]).wait()
                for i in range(sets):

                    @pl.when(tier == 0)
                    def _():
                        for one in loads[i]:
                            one.wait()

                    out[i][tier] = jnp.dot(
                        x[tier], held[i][...], preferred_element_type=jnp.float32
                    ).astype(out[i].dtype)
                for t in range(batch):

                    @pl.when(tier == t)
                    def _():
                        for store in stores(t):
                            store.start()

        for tier in range(batch):

            @pl.when(alive[tier])
            def _():
                for store in stores(tier):
                    store.wait()

    found = pl.pallas_call(
        body,
        in_specs=[SMEM] + [ANY] * (1 + len(flat) + len(after)),
        out_specs=[ANY] * (sets * batch + more),
        out_shape=[
            jax.ShapeDtypeStruct((span, size), jnp.bfloat16) for size in widths for _ in range(batch)
        ]
        + [jax.ShapeDtypeStruct((shared, span, widths[0]), jnp.bfloat16)] * more,
        scratch_shapes=[pltpu.VMEM((batch, span, width), jnp.bfloat16)]
        + [pltpu.VMEM((width, size), jnp.bfloat16) for size in widths]
        + [pltpu.VMEM((batch, span, size), jnp.bfloat16) for size in widths]
        + [
            pltpu.SemaphoreType.DMA((batch,)),
            pltpu.SemaphoreType.DMA((len(flat),)),
            pltpu.SemaphoreType.DMA((sets + 1, batch)),
        ],
        compiler_params=pltpu.CompilerParams(vmem_limit_bytes=ROOM),
        cost_estimate=cost(2 * batch * span * width * sum(widths), 8 << 20),
    )(lengths, rows, *flat, *after)
    return [found[i * batch : (i + 1) * batch] for i in range(sets)], found[-1]


def attend(tiers, columns, lengths, chosen, queries, own_kv, slabs, wo, parts):
    group = len(tiers)
    span, q_width = queries[0].shape
    blocks = span // KB
    kv_width = own_kv[0].shape[-1] // 2
    kv_heads = kv_width // HD
    per = q_width // kv_width
    width = wo.shape[1]
    piece = width // (parts * CORES)
    names = chosen.shape[2]
    devices = lax.axis_size("kv")
    most = max(len(part) for part in slabs)
    room = (most + 1) * blocks
    arrays = [array for part in slabs for array, _, _, _ in part]

    def body(len_ref, pick_ref, names_ref, *rest):
        q_hbm, kv_hbm = rest[:group], rest[group : 2 * group]
        rest = rest[2 * group :]
        slab_refs = rest[: len(arrays)]
        w_hbm = rest[len(arrays)]
        rest = rest[len(arrays) + 1 :]
        keep_hbm, give_hbm, q_ref, w_ref, packed, top, low, acc, att, mask, out = rest[:11]
        marks, listed, count, q_sem, kv_sem, w_sem, slot_sem, out_sem = rest[11:]
        here = lax.axis_index("kv")
        member = lax.axis_index("tp")
        y, core = lax.div(member, CORES), lax.rem(member, CORES)
        row, column = lax.div(here, columns), lax.rem(here, columns)
        load_w = pltpu.make_async_copy(w_hbm, w_ref, w_sem)
        any_alive = here * span < len_ref[nth_longest(len_ref, min(tiers))]

        @pl.when(any_alive)
        def _():
            load_w.start()

        def stores(g, side, far):
            return pltpu.make_async_copy(
                out.at[g, side, far],
                (give_hbm, keep_hbm)[side].at[far, g],
                out_sem.at[g, side, far],
            )

        def load(g):
            for i in range(group):

                @pl.when(g == i)
                def _():
                    pltpu.make_async_copy(q_hbm[i], q_ref, q_sem).start()
                    pltpu.make_async_copy(kv_hbm[i], packed.at[pl.ds(0, span)], kv_sem).start()

        def one(g, tier):
            seq = nth_longest(len_ref, tier)
            length = len_ref[seq]

            @pl.when(here * span < length)
            def _():
                opening = (g == 0) | (here * span >= len_ref[nth_longest(len_ref, tier + 1)])

                @pl.when(opening)
                def _():
                    load(g)

                for c in range(blocks):
                    listed[c] = here * blocks + c
                count[0] = blocks
                if arrays:

                    @pl.when(here > 0)
                    def _():
                        @pl.loop(0, devices * blocks, unroll=8)
                        def _(b):
                            marks[b] = 0

                        @pl.loop(0, names, unroll=4)
                        def _(t):
                            for i in range(blocks):
                                marks[pick_ref[seq, i, t]] = 1

                    at = 0
                    for i in range(group):
                        for _, place, back, turned in slabs[i]:
                            ref = slab_refs[at] if place is None else slab_refs[at].at[place]
                            at += 1
                            source = (row - back) * columns + lax.rem(
                                column - turned + columns, columns
                            )

                            @pl.when((g == i) & (row >= back) & (source < here))
                            def _():
                                @pl.loop(0, blocks)
                                def _(c):
                                    @pl.when(marks[source * blocks + c] > 0)
                                    def _():
                                        slot = count[0]
                                        listed[slot] = source * blocks + c
                                        count[0] = slot + 1
                                        pltpu.make_async_copy(
                                            ref.at[pl.ds(pl.multiple_of(c * KB, KB), KB)],
                                            packed.at[pl.ds(pl.multiple_of(slot * KB, KB), KB)],
                                            slot_sem.at[slot],
                                        ).start()

                widen = lax.broadcasted_iota(jnp.int32, (blocks, span), 1) // KB
                widen = widen == lax.broadcasted_iota(jnp.int32, (blocks, span), 0)
                picked = lax.dot_general(
                    names_ref[seq].astype(jnp.float32),
                    widen.astype(jnp.float32),
                    (((0,), (0,)), ((), ())),
                    precision=lax.Precision.HIGHEST,
                    preferred_element_type=jnp.float32,
                )
                picked = jnp.round(picked).astype(jnp.int32)
                own_id = here * blocks + lax.broadcasted_iota(jnp.int32, (1, span), 1) // KB
                times = jnp.sum((picked == own_id).astype(jnp.float32), axis=0, keepdims=True)
                extra = jnp.log2(times) * (1.0 / SCALE)
                top[...] = jnp.full_like(top, -jnp.inf)
                low[...] = jnp.zeros_like(low)
                acc[...] = jnp.zeros_like(acc)
                pltpu.make_async_copy(q_hbm[0], q_ref, q_sem).wait()
                pltpu.make_async_copy(kv_hbm[0], packed.at[pl.ds(0, span)], kv_sem).wait()
                found = count[0]
                chunks = lax.div(found + blocks - 1, blocks)

                @pl.loop(0, chunks)
                def _(chunk):
                    @pl.when(chunk == 1)
                    def _():
                        @pl.loop(found, chunks * blocks)
                        def _(slot):
                            listed[slot] = -1
                            packed[pl.ds(pl.multiple_of(slot * KB, KB), KB), :] = jnp.zeros(
                                (KB, 2 * kv_width), packed.dtype
                            )

                        @pl.loop(blocks, found)
                        def _(slot):
                            pltpu.make_async_copy(
                                kv_hbm[0].at[pl.ds(0, KB)],
                                packed.at[pl.ds(pl.multiple_of(slot * KB, KB), KB)],
                                slot_sem.at[slot],
                            ).wait()

                    query = lax.broadcasted_iota(jnp.int32, (KB, span), 1)
                    for c in range(blocks):
                        named = picked == listed[chunk * blocks + c]
                        named = jnp.max(jnp.where(named, 0.0, -jnp.inf), axis=0, keepdims=True)
                        key = c * KB + lax.broadcasted_iota(jnp.int32, (KB, span), 0)
                        key = jnp.where(chunk == 0, key, -1)
                        part = jnp.where(key == query, extra, named)
                        mask[c] = jnp.where(key <= query, part, -jnp.inf)
                    at = pl.ds(pl.multiple_of(chunk * span, span), span)
                    for head in range(kv_heads):
                        base = head * per * HD
                        rows = jnp.concatenate(
                            [q_ref[:, base + k * HD : base + (k + 1) * HD] for k in range(per)],
                            axis=0,
                        )
                        s = lax.dot_general(
                            packed[at, head * HD : (head + 1) * HD],
                            rows,
                            (((1,), (1,)), ((), ())),
                            preferred_element_type=jnp.float32,
                        )
                        bias = mask[...].reshape(span, span)
                        s = s + jnp.concatenate([bias] * per, axis=1)
                        old = top[head]
                        high = jnp.maximum(old, jnp.max(s, axis=0, keepdims=True))
                        e = jnp.exp2((s - high) * SCALE)
                        fade = jnp.exp2((old - high) * SCALE)
                        top[head] = high
                        low[head] = low[head] * fade + jnp.sum(e, axis=0, keepdims=True)
                        acc[head] = acc[head] * fade + lax.dot_general(
                            packed[at, kv_width + head * HD : kv_width + (head + 1) * HD],
                            e.astype(jnp.bfloat16),
                            (((0,), (0,)), ((), ())),
                            preferred_element_type=jnp.float32,
                        )

                load(g + 1)
                living = here * span + lax.broadcasted_iota(jnp.int32, (span, 1), 0) < length
                for head in range(kv_heads):
                    done = acc[head] * (1.0 / low[head])
                    for k in range(per):
                        col = (head * per + k) * HD
                        att[:, col : col + HD] = jnp.where(
                            living, done[:, k * span : (k + 1) * span].T, 0.0
                        ).astype(att.dtype)

                @pl.when(opening)
                def _():
                    load_w.wait()

                for side in range(CORES):
                    mine = (CORES - 1 - core, core)[side]

                    @pl.loop(0, parts)
                    def _(step):
                        far = parts - 1 - step
                        first = (lax.rem(y + far, parts) * CORES + mine) * piece
                        out[g, side, far] = jnp.dot(
                            att[...],
                            w_ref[:, pl.ds(pl.multiple_of(first, piece), piece)],
                            preferred_element_type=jnp.float32,
                        ).astype(out.dtype)
                        stores(g, side, far).start()

        if group == 1:
            one(0, tiers[0])
        else:

            @pl.loop(0, group)
            def _(g):
                one(g, tiers[0] - g)

        for g in range(group):

            @pl.when(here * span < len_ref[nth_longest(len_ref, tiers[g])])
            def _():
                for side in range(CORES):
                    for far in range(parts):
                        stores(g, side, far).wait()

    result = jax.ShapeDtypeStruct((parts, group, span, piece), jnp.bfloat16)
    return pl.pallas_call(
        body,
        in_specs=[SMEM, SMEM, VMEM, *[ANY] * (2 * group + len(arrays) + 1)],
        out_specs=[ANY, ANY],
        out_shape=[result, result],
        scratch_shapes=[
            pltpu.VMEM((span, q_width), jnp.bfloat16),
            pltpu.VMEM(wo.shape, jnp.bfloat16),
            pltpu.VMEM((room * KB, 2 * kv_width), jnp.bfloat16),
            pltpu.VMEM((kv_heads, 1, per * span), jnp.float32),
            pltpu.VMEM((kv_heads, 1, per * span), jnp.float32),
            pltpu.VMEM((kv_heads, HD, per * span), jnp.float32),
            pltpu.VMEM((span, q_width), jnp.bfloat16),
            pltpu.VMEM((blocks, KB, span), jnp.float32),
            pltpu.VMEM((group, CORES, parts, span, piece), jnp.bfloat16),
            pltpu.SMEM((devices * blocks,), jnp.int32),
            pltpu.SMEM((room,), jnp.int32),
            pltpu.SMEM((1,), jnp.int32),
            pltpu.SemaphoreType.DMA,
            pltpu.SemaphoreType.DMA,
            pltpu.SemaphoreType.DMA,
            pltpu.SemaphoreType.DMA((room,)),
            pltpu.SemaphoreType.DMA((group, CORES, parts)),
        ],
        compiler_params=pltpu.CompilerParams(vmem_limit_bytes=ROOM),
        cost_estimate=cost(group * 4 * span * q_width * width, group * (3 << 20)),
    )(lengths, chosen, chosen, *queries, *own_kv, *arrays, wo)


def finish(lengths, batch, groups, before=None):
    _, span, piece = groups[0][1].shape
    parts = 1 + len(groups[0][2])
    every = [(tier, g, at) for at, group in enumerate(groups) for g, tier in enumerate(group[0])]
    each = parts

    def body(len_ref, *refs):
        given = refs[: each * len(groups)]
        out_ref, nears, terms, sums, in_sem, out_sem = refs[-6:]
        here = lax.axis_index("kv")
        seqs = [nth_longest(len_ref, tier) for tier, _, _ in every]

        def loads(n):
            _, g, at = every[n]
            mine = given[at * each : (at + 1) * each]
            return [pltpu.make_async_copy(mine[0].at[g], nears.at[n], in_sem.at[n, 0])] + [
                pltpu.make_async_copy(ref.at[g], terms.at[n, i], in_sem.at[n, 1 + i])
                for i, ref in enumerate(mine[1:])
            ]

        def store(n):
            return pltpu.make_async_copy(sums.at[n], out_ref.at[seqs[n]], out_sem.at[n])

        for n in range(len(every)):

            @pl.when(here * span < len_ref[seqs[n]])
            def _():
                for load in loads(n):
                    load.start()

        for n in range(len(every)):
            alive = here * span < len_ref[seqs[n]]

            @pl.when(alive)
            def _():
                for load in loads(n):
                    load.wait()
                total = nears[n]
                for i in range(each - 1):
                    total = total + terms[n, i].astype(jnp.float32)
                sums[n] = total.astype(sums.dtype)

            @pl.when(jnp.logical_not(alive))
            def _():
                sums[n] = jnp.zeros((span, piece), sums.dtype)

            store(n).start()
        for n in range(len(every)):
            store(n).wait()

    operands = [part for _, near, coming in groups for part in (near, *coming)]
    aliases = {}
    if before is not None:
        aliases = {1 + len(operands): 0}
        operands.append(before)
    return pl.pallas_call(
        body,
        in_specs=[SMEM] + [ANY] * len(operands),
        out_specs=ANY,
        out_shape=jax.ShapeDtypeStruct((batch, span, piece), jnp.bfloat16),
        scratch_shapes=[
            pltpu.VMEM((len(every), span, piece), jnp.float32),
            pltpu.VMEM((len(every), each, span, piece), jnp.bfloat16),
            pltpu.VMEM((len(every), span, piece), jnp.bfloat16),
            pltpu.SemaphoreType.DMA((len(every), each)),
            pltpu.SemaphoreType.DMA((len(every),)),
        ],
        input_output_aliases=aliases,
        compiler_params=pltpu.CompilerParams(vmem_limit_bytes=ROOM),
        cost_estimate=cost(len(every) * 4 * span * piece, len(every) * 8 * span * piece),
        name="finish",
    )(lengths, *operands)


def gather_spans(slabs, joined, first, reaches, columns):
    arrived = [[] for _ in reaches]

    def turn(x, back, rows):
        found = []
        for d in range(1, columns):
            pairs = [
                (r * columns + c, r * columns + (c + d) % columns)
                for r in range(back, rows)
                for c in range(columns)
                if r > 0 or c + d < columns
            ]
            found.append((lax.ppermute(x, "kv", pairs), d))
        return found

    for moved, d in turn(joined, 0, reaches[first] // columns):
        for place in range(joined.shape[0]):
            arrived[first + place].append((moved, place, 0, d))
    for tier, reach in enumerate(reaches):
        rows = reach // columns
        if reach > 1 and not first <= tier < first + joined.shape[0]:
            for moved, d in turn(slabs[tier], 0, rows):
                arrived[tier].append((moved, None, 0, d))
        passing = slabs[tier]
        for back in range(1, rows):
            pairs = [
                (r * columns + c, (r + 1) * columns + c)
                for r in range(back - 1, rows - 1)
                for c in range(columns)
            ]
            passing = lax.ppermute(passing, "kv", pairs)
            arrived[tier].append((passing, None, back, 0))
            for moved, d in turn(passing, back, rows):
                arrived[tier].append((moved, None, back, d))
    return arrived


def layer(reaches, together, columns, inputs, wq, wk, wv, wo, chosen, lengths):
    batch, _, _ = inputs.shape
    members = lax.axis_size("tp")
    parts = members // CORES

    first = 1
    shared = sum(reach > 1 for reach in reaches) - first
    (own, queries), joined = project(lengths, inputs, ((wk, wv), (wq,)), first, shared)
    gathered = gather_spans(own, joined, first, reaches, columns)

    groups = []
    for tiers in together:
        reach = max(max(reaches[tier] for tier in tiers), 1)
        keep, give = attend(
            tiers,
            columns,
            lengths,
            chosen,
            [queries[tier] for tier in tiers],
            [own[tier] for tier in tiers],
            [gathered[tier] for tier in tiers],
            wo,
            parts,
        )

        def swap(x, move):
            pairs = [
                (k * members + t, k * members + move(t))
                for k in range(reach)
                for t in range(members)
            ]
            return lax.ppermute(x, ("kv", "tp"), pairs)

        got = swap(give, lambda t: t ^ 1)
        coming = []
        for far in range(1, parts):
            both = keep[far].astype(jnp.float32) + got[far].astype(jnp.float32)
            coming.append(
                swap(
                    both.astype(jnp.bfloat16),
                    lambda t, far=far: ((t // CORES + far) % parts) * CORES + t % CORES,
                )
            )
        near = keep[0].astype(jnp.float32) + got[0].astype(jnp.float32)
        groups.append((tiers, near, coming))
    out = None
    if len(groups) > 1:
        out = finish(lengths, batch, groups[:-1])
    return finish(lengths, batch, groups[-1:], out)


def tier_reaches(devices, batch, columns):
    reaches = []
    for tier in range(batch):
        reach = devices >> tier
        if reach > 1:
            reach = -(-reach // columns) * columns
        reaches.append(reach)
    return tuple(reaches)


def solution(mesh):
    placed = (
        P(None, "kv", None),
        P(None, "tp"),
        P(None, "tp"),
        P(None, "tp"),
        P("tp", None),
        P(None, "kv", None),
        P(),
    )
    devices = mesh.shape["kv"]
    columns = 1 << ((devices.bit_length() - 1) // 2)

    def shards(*args):
        batch, span = args[0].shape[0], args[0].shape[1]
        lengths = args[-1]
        common = tier_reaches(devices, batch, columns)
        backwards = range(batch - 1, -1, -1)
        together = (tuple(backwards[:1]), tuple(backwards[1:-1]), tuple(backwards[-1:]))
        out = layer(common, together, columns, *args)
        reach = jnp.array(common, jnp.int32)
        longer = jnp.sum((lengths[None, :] > reach[:, None] * span).astype(jnp.int32), axis=1)
        fits = jnp.all(longer <= jnp.arange(batch, dtype=jnp.int32))
        return lax.cond(
            fits,
            lambda done, *a: done,
            lambda done, *a: layer((devices,) * batch, (tuple(backwards),), columns, *a),
            out,
            *args,
        )

    return jax.shard_map(
        shards, mesh=mesh, in_specs=placed, out_specs=P(None, "kv", "tp"), check_vma=False
    )
```

```python
import math

import jax
import jax.numpy as jnp
from jax import lax
from jax.experimental import pallas as pl
from jax.experimental.pallas import tpu as pltpu
from jax.sharding import PartitionSpec as P

HD = 128
KB = 64
CORES = 2
ROOM = 24 << 20
SCALE = HD ** (-0.5) * math.log2(math.e)


ANY = pl.BlockSpec(memory_space=pl.ANY)
SMEM = pl.BlockSpec(memory_space=pltpu.SMEM)
VMEM = pl.BlockSpec(memory_space=pltpu.VMEM)


def nth_longest(len_ref, tier):
    batch = len_ref.shape[0]
    found = jnp.int32(0)
    for b in range(batch):
        rank = jnp.int32(0)
        for other in range(batch):
            if other < b:
                rank += (len_ref[other] >= len_ref[b]).astype(jnp.int32)
            elif other > b:
                rank += (len_ref[other] > len_ref[b]).astype(jnp.int32)
        found = jnp.where(rank == tier, b, found)
    return found


def cost(flops, moved):
    return pl.CostEstimate(flops=int(flops), bytes_accessed=int(moved), transcendentals=0)


def project(lengths, rows, weights, first=0, shared=0, after=()):
    batch, span, width = rows.shape
    sets = len(weights)
    widths = [sum(w.shape[1] for w in part) for part in weights]
    flat = [w for part in weights for w in part]
    more = min(shared, 1)

    def body(len_ref, x_ref, *refs):
        given, refs = refs[: len(flat)], refs[len(flat) + len(after) :]
        outs, refs = refs[: sets * batch], refs[sets * batch :]
        again, refs = refs[:more], refs[more:]
        x, refs = refs[0], refs[1:]
        held, out, (sem, w_sem, out_sem) = refs[:sets], refs[sets : 2 * sets], refs[2 * sets :]
        here = lax.axis_index("kv")
        seqs = [nth_longest(len_ref, tier) for tier in range(batch)]
        alive = [here * span < len_ref[seq] for seq in seqs]
        loads, at = [], 0
        for i, part in enumerate(weights):
            loads.append([])
            base = 0
            for w in part:
                loads[i].append(
                    pltpu.make_async_copy(
                        given[at], held[i].at[:, pl.ds(base, w.shape[1])], w_sem.at[at]
                    )
                )
                at += 1
                base += w.shape[1]

        def load(tier):
            return pltpu.make_async_copy(x_ref.at[seqs[tier]], x.at[tier], sem.at[tier])

        def stores(tier):
            found = [
                pltpu.make_async_copy(
                    out[i].at[tier], outs[i * batch + tier], out_sem.at[i, tier]
                )
                for i in range(sets)
            ]
            if first <= tier < first + shared:
                found.append(
                    pltpu.make_async_copy(
                        out[0].at[tier], again[0].at[tier - first], out_sem.at[sets, tier]
                    )
                )
            return found

        @pl.when(alive[0])
        def _():
            for one in loads[0]:
                one.start()
            load(0).start()
            for part in loads[1:]:
                for one in part:
                    one.start()

        for tier in range(1, batch):

            @pl.when(alive[tier])
            def _():
                load(tier).start()

        @pl.loop(0, batch)
        def _(tier):
            @pl.when(here * span < len_ref[nth_longest(len_ref, tier)])
            def _():
                pltpu.make_async_copy(x_ref.at[0], x.at[tier], sem.at[tier]).wait()
                for i in range(sets):

                    @pl.when(tier == 0)
                    def _():
                        for one in loads[i]:
                            one.wait()

                    out[i][tier] = jnp.dot(
                        x[tier], held[i][...], preferred_element_type=jnp.float32
                    ).astype(out[i].dtype)
                for t in range(batch):

                    @pl.when(tier == t)
                    def _():
                        for store in stores(t):
                            store.start()

        for tier in range(batch):

            @pl.when(alive[tier])
            def _():
                for store in stores(tier):
                    store.wait()

    found = pl.pallas_call(
        body,
        in_specs=[SMEM] + [ANY] * (1 + len(flat) + len(after)),
        out_specs=[ANY] * (sets * batch + more),
        out_shape=[
            jax.ShapeDtypeStruct((span, size), jnp.bfloat16) for size in widths for _ in range(batch)
        ]
        + [jax.ShapeDtypeStruct((shared, span, widths[0]), jnp.bfloat16)] * more,
        scratch_shapes=[pltpu.VMEM((batch, span, width), jnp.bfloat16)]
        + [pltpu.VMEM((width, size), jnp.bfloat16) for size in widths]
        + [pltpu.VMEM((batch, span, size), jnp.bfloat16) for size in widths]
        + [
            pltpu.SemaphoreType.DMA((batch,)),
            pltpu.SemaphoreType.DMA((len(flat),)),
            pltpu.SemaphoreType.DMA((sets + 1, batch)),
        ],
        compiler_params=pltpu.CompilerParams(vmem_limit_bytes=ROOM),
        cost_estimate=cost(2 * batch * span * width * sum(widths), 8 << 20),
    )(lengths, rows, *flat, *after)
    return [found[i * batch : (i + 1) * batch] for i in range(sets)], found[-1]


def attend(tiers, columns, lengths, chosen, queries, own_kv, slabs, wo, parts):
    group = len(tiers)
    span, q_width = queries[0].shape
    blocks = span // KB
    kv_width = own_kv[0].shape[-1] // 2
    kv_heads = kv_width // HD
    per = q_width // kv_width
    width = wo.shape[1]
    piece = width // (parts * CORES)
    names = chosen.shape[2]
    devices = lax.axis_size("kv")
    most = max(len(part) for part in slabs)
    room = (most + 1) * blocks
    arrays = [array for part in slabs for array, _, _, _ in part]

    def body(len_ref, pick_ref, names_ref, *rest):
        q_hbm, kv_hbm = rest[:group], rest[group : 2 * group]
        rest = rest[2 * group :]
        slab_refs = rest[: len(arrays)]
        w_hbm = rest[len(arrays)]
        rest = rest[len(arrays) + 1 :]
        keep_hbm, give_hbm, q_ref, w_ref, packed, top, low, acc, att, mask, out = rest[:11]
        marks, listed, count, q_sem, kv_sem, w_sem, slot_sem, out_sem = rest[11:]
        here = lax.axis_index("kv")
        member = lax.axis_index("tp")
        y, core = lax.div(member, CORES), lax.rem(member, CORES)
        row, column = lax.div(here, columns), lax.rem(here, columns)
        load_w = pltpu.make_async_copy(w_hbm, w_ref, w_sem)
        any_alive = here * span < len_ref[nth_longest(len_ref, min(tiers))]

        @pl.when(any_alive)
        def _():
            load_w.start()

        def stores(g, side, far):
            return pltpu.make_async_copy(
                out.at[g, side, far],
                (give_hbm, keep_hbm)[side].at[far, g],
                out_sem.at[g, side, far],
            )

        def load(g):
            for i in range(group):

                @pl.when(g == i)
                def _():
                    pltpu.make_async_copy(q_hbm[i], q_ref, q_sem).start()
                    pltpu.make_async_copy(kv_hbm[i], packed.at[pl.ds(0, span)], kv_sem).start()

        def one(g, tier):
            seq = nth_longest(len_ref, tier)
            length = len_ref[seq]

            @pl.when(here * span < length)
            def _():
                opening = (g == 0) | (here * span >= len_ref[nth_longest(len_ref, tier + 1)])

                @pl.when(opening)
                def _():
                    load(g)

                for c in range(blocks):
                    listed[c] = here * blocks + c
                count[0] = blocks
                if arrays:

                    @pl.when(here > 0)
                    def _():
                        @pl.loop(0, devices * blocks, unroll=8)
                        def _(b):
                            marks[b] = 0

                        @pl.loop(0, names, unroll=4)
                        def _(t):
                            for i in range(blocks):
                                marks[pick_ref[seq, i, t]] = 1

                    at = 0
                    for i in range(group):
                        for _, place, back, turned in slabs[i]:
                            ref = slab_refs[at] if place is None else slab_refs[at].at[place]
                            at += 1
                            source = (row - back) * columns + lax.rem(
                                column - turned + columns, columns
                            )

                            @pl.when((g == i) & (row >= back) & (source < here))
                            def _():
                                @pl.loop(0, blocks)
                                def _(c):
                                    @pl.when(marks[source * blocks + c] > 0)
                                    def _():
                                        slot = count[0]
                                        listed[slot] = source * blocks + c
                                        count[0] = slot + 1
                                        pltpu.make_async_copy(
                                            ref.at[pl.ds(pl.multiple_of(c * KB, KB), KB)],
                                            packed.at[pl.ds(pl.multiple_of(slot * KB, KB), KB)],
                                            slot_sem.at[slot],
                                        ).start()

                widen = lax.broadcasted_iota(jnp.int32, (blocks, span), 1) // KB
                widen = widen == lax.broadcasted_iota(jnp.int32, (blocks, span), 0)
                picked = lax.dot_general(
                    names_ref[seq].astype(jnp.float32),
                    widen.astype(jnp.float32),
                    (((0,), (0,)), ((), ())),
                    precision=lax.Precision.HIGHEST,
                    preferred_element_type=jnp.float32,
                )
                picked = jnp.round(picked).astype(jnp.int32)
                own_id = here * blocks + lax.broadcasted_iota(jnp.int32, (1, span), 1) // KB
                times = jnp.sum((picked == own_id).astype(jnp.float32), axis=0, keepdims=True)
                extra = jnp.log2(times) * (1.0 / SCALE)
                top[...] = jnp.full_like(top, -jnp.inf)
                low[...] = jnp.zeros_like(low)
                acc[...] = jnp.zeros_like(acc)
                pltpu.make_async_copy(q_hbm[0], q_ref, q_sem).wait()
                pltpu.make_async_copy(kv_hbm[0], packed.at[pl.ds(0, span)], kv_sem).wait()
                found = count[0]
                chunks = lax.div(found + blocks - 1, blocks)

                @pl.loop(0, chunks)
                def _(chunk):
                    @pl.when(chunk == 1)
                    def _():
                        @pl.loop(found, chunks * blocks)
                        def _(slot):
                            listed[slot] = -1
                            packed[pl.ds(pl.multiple_of(slot * KB, KB), KB), :] = jnp.zeros(
                                (KB, 2 * kv_width), packed.dtype
                            )

                        @pl.loop(blocks, found)
                        def _(slot):
                            pltpu.make_async_copy(
                                kv_hbm[0].at[pl.ds(0, KB)],
                                packed.at[pl.ds(pl.multiple_of(slot * KB, KB), KB)],
                                slot_sem.at[slot],
                            ).wait()

                    query = lax.broadcasted_iota(jnp.int32, (KB, span), 1)
                    for c in range(blocks):
                        named = picked == listed[chunk * blocks + c]
                        named = jnp.max(jnp.where(named, 0.0, -jnp.inf), axis=0, keepdims=True)
                        key = c * KB + lax.broadcasted_iota(jnp.int32, (KB, span), 0)
                        key = jnp.where(chunk == 0, key, -1)
                        part = jnp.where(key == query, extra, named)
                        mask[c] = jnp.where(key <= query, part, -jnp.inf)
                    at = pl.ds(pl.multiple_of(chunk * span, span), span)
                    for head in range(kv_heads):
                        base = head * per * HD
                        rows = jnp.concatenate(
                            [q_ref[:, base + k * HD : base + (k + 1) * HD] for k in range(per)],
                            axis=0,
                        )
                        s = lax.dot_general(
                            packed[at, head * HD : (head + 1) * HD],
                            rows,
                            (((1,), (1,)), ((), ())),
                            preferred_element_type=jnp.float32,
                        )
                        bias = mask[...].reshape(span, span)
                        s = s + jnp.concatenate([bias] * per, axis=1)
                        old = top[head]
                        high = jnp.maximum(old, jnp.max(s, axis=0, keepdims=True))
                        e = jnp.exp2((s - high) * SCALE)
                        fade = jnp.exp2((old - high) * SCALE)
                        top[head] = high
                        low[head] = low[head] * fade + jnp.sum(e, axis=0, keepdims=True)
                        acc[head] = acc[head] * fade + lax.dot_general(
                            packed[at, kv_width + head * HD : kv_width + (head + 1) * HD],
                            e.astype(jnp.bfloat16),
                            (((0,), (0,)), ((), ())),
                            preferred_element_type=jnp.float32,
                        )

                load(g + 1)
                living = here * span + lax.broadcasted_iota(jnp.int32, (span, 1), 0) < length
                for head in range(kv_heads):
                    done = acc[head] * (1.0 / low[head])
                    for k in range(per):
                        col = (head * per + k) * HD
                        att[:, col : col + HD] = jnp.where(
                            living, done[:, k * span : (k + 1) * span].T, 0.0
                        ).astype(att.dtype)

                @pl.when(opening)
                def _():
                    load_w.wait()

                for side in range(CORES):
                    mine = (CORES - 1 - core, core)[side]

                    @pl.loop(0, parts)
                    def _(step):
                        far = parts - 1 - step
                        first = (lax.rem(y + far, parts) * CORES + mine) * piece
                        out[g, side, far] = jnp.dot(
                            att[...],
                            w_ref[:, pl.ds(pl.multiple_of(first, piece), piece)],
                            preferred_element_type=jnp.float32,
                        ).astype(out.dtype)
                        stores(g, side, far).start()

        if group == 1:
            one(0, tiers[0])
        else:

            @pl.loop(0, group)
            def _(g):
                one(g, tiers[0] - g)

        for g in range(group):

            @pl.when(here * span < len_ref[nth_longest(len_ref, tiers[g])])
            def _():
                for side in range(CORES):
                    for far in range(parts):
                        stores(g, side, far).wait()

    result = jax.ShapeDtypeStruct((parts, group, span, piece), jnp.bfloat16)
    return pl.pallas_call(
        body,
        in_specs=[SMEM, SMEM, VMEM, *[ANY] * (2 * group + len(arrays) + 1)],
        out_specs=[ANY, ANY],
        out_shape=[result, result],
        scratch_shapes=[
            pltpu.VMEM((span, q_width), jnp.bfloat16),
            pltpu.VMEM(wo.shape, jnp.bfloat16),
            pltpu.VMEM((room * KB, 2 * kv_width), jnp.bfloat16),
            pltpu.VMEM((kv_heads, 1, per * span), jnp.float32),
            pltpu.VMEM((kv_heads, 1, per * span), jnp.float32),
            pltpu.VMEM((kv_heads, HD, per * span), jnp.float32),
            pltpu.VMEM((span, q_width), jnp.bfloat16),
            pltpu.VMEM((blocks, KB, span), jnp.float32),
            pltpu.VMEM((group, CORES, parts, span, piece), jnp.bfloat16),
            pltpu.SMEM((devices * blocks,), jnp.int32),
            pltpu.SMEM((room,), jnp.int32),
            pltpu.SMEM((1,), jnp.int32),
            pltpu.SemaphoreType.DMA,
            pltpu.SemaphoreType.DMA,
            pltpu.SemaphoreType.DMA,
            pltpu.SemaphoreType.DMA((room,)),
            pltpu.SemaphoreType.DMA((group, CORES, parts)),
        ],
        compiler_params=pltpu.CompilerParams(vmem_limit_bytes=ROOM),
        cost_estimate=cost(group * 4 * span * q_width * width, group * (3 << 20)),
    )(lengths, chosen, chosen, *queries, *own_kv, *arrays, wo)


def finish(lengths, batch, groups, before=None):
    _, span, piece = groups[0][1].shape
    parts = 1 + len(groups[0][2])
    every = [(tier, g, at) for at, group in enumerate(groups) for g, tier in enumerate(group[0])]
    each = parts

    def body(len_ref, *refs):
        given = refs[: each * len(groups)]
        out_ref, nears, terms, sums, in_sem, out_sem = refs[-6:]
        here = lax.axis_index("kv")
        seqs = [nth_longest(len_ref, tier) for tier, _, _ in every]

        def loads(n):
            _, g, at = every[n]
            mine = given[at * each : (at + 1) * each]
            return [pltpu.make_async_copy(mine[0].at[g], nears.at[n], in_sem.at[n, 0])] + [
                pltpu.make_async_copy(ref.at[g], terms.at[n, i], in_sem.at[n, 1 + i])
                for i, ref in enumerate(mine[1:])
            ]

        def store(n):
            return pltpu.make_async_copy(sums.at[n], out_ref.at[seqs[n]], out_sem.at[n])

        for n in range(len(every)):

            @pl.when(here * span < len_ref[seqs[n]])
            def _():
                for load in loads(n):
                    load.start()

        for n in range(len(every)):
            alive = here * span < len_ref[seqs[n]]

            @pl.when(alive)
            def _():
                for load in loads(n):
                    load.wait()
                total = nears[n]
                for i in range(each - 1):
                    total = total + terms[n, i].astype(jnp.float32)
                sums[n] = total.astype(sums.dtype)

            @pl.when(jnp.logical_not(alive))
            def _():
                sums[n] = jnp.zeros((span, piece), sums.dtype)

            store(n).start()
        for n in range(len(every)):
            store(n).wait()

    operands = [part for _, near, coming in groups for part in (near, *coming)]
    aliases = {}
    if before is not None:
        aliases = {1 + len(operands): 0}
        operands.append(before)
    return pl.pallas_call(
        body,
        in_specs=[SMEM] + [ANY] * len(operands),
        out_specs=ANY,
        out_shape=pltpu.HBM((batch, span, piece), jnp.bfloat16),
        scratch_shapes=[
            pltpu.VMEM((len(every), span, piece), jnp.float32),
            pltpu.VMEM((len(every), each, span, piece), jnp.bfloat16),
            pltpu.VMEM((len(every), span, piece), jnp.bfloat16),
            pltpu.SemaphoreType.DMA((len(every), each)),
            pltpu.SemaphoreType.DMA((len(every),)),
        ],
        input_output_aliases=aliases,
        compiler_params=pltpu.CompilerParams(vmem_limit_bytes=ROOM),
        cost_estimate=cost(len(every) * 4 * span * piece, len(every) * 8 * span * piece),
        name="finish",
    )(lengths, *operands)


def gather_spans(slabs, joined, first, reaches, columns):
    arrived = [[] for _ in reaches]

    def turn(x, back, rows):
        found = []
        for d in range(1, columns):
            pairs = [
                (r * columns + c, r * columns + (c + d) % columns)
                for r in range(back, rows)
                for c in range(columns)
                if r > 0 or c + d < columns
            ]
            found.append((lax.ppermute(x, "kv", pairs), d))
        return found

    for moved, d in turn(joined, 0, reaches[first] // columns):
        for place in range(joined.shape[0]):
            arrived[first + place].append((moved, place, 0, d))
    for tier, reach in enumerate(reaches):
        rows = reach // columns
        if reach > 1 and not first <= tier < first + joined.shape[0]:
            for moved, d in turn(slabs[tier], 0, rows):
                arrived[tier].append((moved, None, 0, d))
        passing = slabs[tier]
        for back in range(1, rows):
            pairs = [
                (r * columns + c, (r + 1) * columns + c)
                for r in range(back - 1, rows - 1)
                for c in range(columns)
            ]
            passing = lax.ppermute(passing, "kv", pairs)
            arrived[tier].append((passing, None, back, 0))
            for moved, d in turn(passing, back, rows):
                arrived[tier].append((moved, None, back, d))
    return arrived


def layer(reaches, together, columns, inputs, wq, wk, wv, wo, chosen, lengths):
    batch, _, _ = inputs.shape
    members = lax.axis_size("tp")
    parts = members // CORES

    first = 1
    shared = sum(reach > 1 for reach in reaches) - first
    (own, queries), joined = project(lengths, inputs, ((wk, wv), (wq,)), first, shared)
    gathered = gather_spans(own, joined, first, reaches, columns)

    groups = []
    for tiers in together:
        reach = max(max(reaches[tier] for tier in tiers), 1)
        keep, give = attend(
            tiers,
            columns,
            lengths,
            chosen,
            [queries[tier] for tier in tiers],
            [own[tier] for tier in tiers],
            [gathered[tier] for tier in tiers],
            wo,
            parts,
        )

        def swap(x, move):
            pairs = [
                (k * members + t, k * members + move(t))
                for k in range(reach)
                for t in range(members)
            ]
            return lax.ppermute(x, ("kv", "tp"), pairs)

        got = swap(give, lambda t: t ^ 1)
        coming = []
        for far in range(1, parts):
            both = keep[far].astype(jnp.float32) + got[far].astype(jnp.float32)
            coming.append(
                swap(
                    both.astype(jnp.bfloat16),
                    lambda t, far=far: ((t // CORES + far) % parts) * CORES + t % CORES,
                )
            )
        near = keep[0].astype(jnp.float32) + got[0].astype(jnp.float32)
        groups.append((tiers, near, coming))
    out = None
    if len(groups) > 1:
        out = finish(lengths, batch, groups[:-1])
    return finish(lengths, batch, groups[-1:], out)


def tier_reaches(devices, batch, columns):
    reaches = []
    for tier in range(batch):
        reach = devices >> tier
        if reach > 1:
            reach = -(-reach // columns) * columns
        reaches.append(reach)
    return tuple(reaches)


def solution(mesh):
    placed = (
        P(None, "kv", None),
        P(None, "tp"),
        P(None, "tp"),
        P(None, "tp"),
        P("tp", None),
        P(None, "kv", None),
        P(),
    )
    devices = mesh.shape["kv"]
    columns = 1 << ((devices.bit_length() - 1) // 2)

    def shards(*args):
        batch, span = args[0].shape[0], args[0].shape[1]
        lengths = args[-1]
        common = tier_reaches(devices, batch, columns)
        backwards = range(batch - 1, -1, -1)
        together = (tuple(backwards[:1]), tuple(backwards[1:-1]), tuple(backwards[-1:]))
        out = layer(common, together, columns, *args)
        reach = jnp.array(common, jnp.int32)
        longer = jnp.sum((lengths[None, :] > reach[:, None] * span).astype(jnp.int32), axis=1)
        fits = jnp.all(longer <= jnp.arange(batch, dtype=jnp.int32))
        return lax.cond(
            fits,
            lambda done, *a: done,
            lambda done, *a: layer((devices,) * batch, (tuple(backwards),), columns, *a),
            out,
            *args,
        )

    return jax.shard_map(
        shards, mesh=mesh, in_specs=placed, out_specs=P(None, "kv", "tp"), check_vma=False
    )
```
